512 devices in a mesh: sp: 16 (over y, x), tp: 32 (over z, core).
Axes of the slice: x: 4, y: 4, z: 16, core: 2. Of those that a mesh axis runs over, the one named last changes fastest.
Arguments:
- stream: bfloat16 [8192, 4096], P('sp', 'tp'), may hold values from -6 to 6
- gain_first: bfloat16 [4096], P('tp'), may hold values from 0.099609375 to 1.8984375
- query_first: bfloat16 [4096, 4096], P('sp', 'tp'), may hold values from -0.09375 to 0.09375
- key_first: bfloat16 [4096, 4096], P('sp', 'tp'), may hold values from -0.09375 to 0.09375
- value_first: bfloat16 [4096, 4096], P('sp', 'tp'), may hold values from -0.09375 to 0.09375
- offset_first: float32 [32, 15, 31], P('tp'), may hold values from -4 to 254
- gain_second: bfloat16 [4096], P('tp'), may hold values from 0.099609375 to 1.8984375
- query_second: bfloat16 [4096, 4096], P('sp', 'tp'), may hold values from -0.09375 to 0.09375
- key_second: bfloat16 [4096, 4096], P('sp', 'tp'), may hold values from -0.09375 to 0.09375
- value_second: bfloat16 [4096, 4096], P('sp', 'tp'), may hold values from -0.09375 to 0.09375
- offset_second: float32 [32, 15, 31], P('tp'), may hold values from -4 to 254
Outputs:
- result: bfloat16 [8192, 4096], P('sp', 'tp')
The draws below stay inside these ranges and needn't reach their ends.
All inputs are finite; a program needn't handle non-finite values.
Results may differ from the reference program's by a relative error of at most 0.008.
Values may be sent and summed in bfloat16 or wider, within the bound.
A program may use at most 64 MiB of HBM per device.

```python
import jax
import jax.numpy as jnp
import numpy as np
from jax import lax

GRID_W = 64
HEAD_DIM = 128
HEADS = 32
D = 4096
TOKENS = 8192


def draw_stream(key, part):
    first, second = jax.random.split(jax.random.fold_in(key, 11))
    blocks = D // HEAD_DIM
    scales = jnp.exp(jax.random.uniform(first, (blocks,), jnp.float32, jnp.log(0.15), jnp.log(1.0)))
    base = jnp.clip(jax.random.normal(second, (TOKENS, D), jnp.float32), -6.0, 6.0)
    return (base * jnp.repeat(scales, HEAD_DIM)[None, :]).astype(jnp.bfloat16)


def draw_table(key):
    base = jnp.clip(jax.random.normal(key, (HEADS, 15, 31), jnp.float32), -4.0, 4.0)
    return base


def draw_offset_first(key, part):
    return draw_table(jax.random.fold_in(key, 21))


def draw_offset_second(key, part):
    return draw_table(jax.random.fold_in(key, 22))


def levels(key, dims, cuts, least, high):
    level = 1.0
    for axis_at, blocks in cuts:
        steps = jax.random.uniform(jax.random.fold_in(jax.random.fold_in(key, 6), axis_at), (blocks,), jnp.float32, least / len(cuts), high / len(cuts))
        level = level * jnp.repeat(jnp.exp(steps), dims[axis_at] // blocks).reshape((-1,) + (1,) * (len(dims) - 1 - axis_at))
    return level


def normal_values(key, shape, scale, bound, cuts=(), held_as=jnp.bfloat16):
    factor_of = levels(key, shape, cuts, -0.22, 0.18) if cuts else 1.0
    values = jax.random.normal(key, shape, jnp.float32) * scale * factor_of
    return jnp.minimum(jnp.maximum(values, -bound), bound).astype(held_as)


def setup_inputs(seed: int = 0) -> dict:
    key_of = jax.random.split(jax.random.key(seed), 12)
    stream = draw_stream(jax.random.fold_in(key_of[11], 71), 0)
    gain_first = jnp.clip(1.0 + 0.18 * jax.random.normal(key_of[1], (D,), jnp.float32), 0.099609375, 1.8984375).astype(jnp.bfloat16)
    query_first = normal_values(key_of[2], (D, D), D ** -0.5, 0.09375, ((0, 16), (1, 32)))
    key_first = normal_values(key_of[3], (D, D), D ** -0.5, 0.09375, ((0, 16), (1, 32)))
    value_first = normal_values(key_of[4], (D, D), D ** -0.5, 0.09375, ((0, 16), (1, 32)))
    offset_first = draw_offset_first(jax.random.fold_in(key_of[11], 71), 0)
    gain_second = jnp.clip(1.0 + 0.18 * jax.random.normal(key_of[6], (D,), jnp.float32), 0.099609375, 1.8984375).astype(jnp.bfloat16)
    query_second = normal_values(key_of[7], (D, D), D ** -0.5, 0.09375, ((0, 16), (1, 32)))
    key_second = normal_values(key_of[8], (D, D), D ** -0.5, 0.09375, ((0, 16), (1, 32)))
    value_second = normal_values(key_of[9], (D, D), D ** -0.5, 0.09375, ((0, 16), (1, 32)))
    offset_second = draw_offset_second(jax.random.fold_in(key_of[11], 71), 0)
    return {"stream": stream, "gain_first": gain_first, "query_first": query_first, "key_first": key_first, "value_first": value_first, "offset_first": offset_first, "gain_second": gain_second, "query_second": query_second, "key_second": key_second, "value_second": value_second, "offset_second": offset_second}


epsilon = 1e-06

def normalize(stream, gain):
    widened = stream.astype(jnp.float32)
    mean_square = lax.optimization_barrier(jnp.mean(widened * widened, axis=-1, keepdims=True))
    return (widened * lax.rsqrt(mean_square + epsilon) * gain.astype(jnp.float32)).astype(jnp.bfloat16)

def attend(query, keys, values, table, row_start, total_rows):
    rows_here, width, heads, head_size = query.shape
    blocks = width // 16
    query_cols = np.arange(width).reshape(blocks, 16)
    window_start = np.clip(query_cols - 8, 0, width - 16)
    key_cols = np.clip(np.arange(blocks) * 16 - 8, 0, width - 32)[:, None] + np.arange(32)
    column_ok = (key_cols[:, None, :] >= window_start[:, :, None]) & (key_cols[:, None, :] < window_start[:, :, None] + 16)
    column_offset = np.clip(key_cols[:, None, :] - query_cols[:, :, None] + 15, 0, 30)
    column_bias = table.astype(jnp.float32)[:, :, column_offset]
    mask = jnp.asarray(column_ok)[None, :, :, None, :]
    factor = head_size ** (-0.5)

    def one_row(index):
        grid_row = row_start + index
        first = jnp.clip(grid_row - 4, 0, total_rows - 8)
        local = first - row_start + 4
        key_block = lax.dynamic_slice_in_dim(keys, local, 8, 0)[:, key_cols].astype(jnp.float32)
        value_block = lax.dynamic_slice_in_dim(values, local, 8, 0)[:, key_cols].astype(jnp.float32)
        query_row = lax.dynamic_index_in_dim(query, index, 0, keepdims=False).reshape(blocks, 16, heads, head_size)
        scores = jnp.einsum('jqhe,mjkhe->hjqmk', query_row.astype(jnp.float32), key_block) * factor
        row_offset = first + jnp.arange(8, dtype=jnp.int32) - grid_row + 7
        row_bias = jnp.transpose(jnp.take(column_bias, row_offset, axis=1), (0, 2, 3, 1, 4))
        scores = jnp.where(mask, scores + row_bias, -1e+30)
        weight = jax.nn.softmax(scores.reshape(heads, blocks, 16, 256), axis=-1)
        rounded = weight.astype(jnp.bfloat16).reshape(heads, blocks, 16, 8, 32)
        output = jnp.einsum('hjqmk,mjkhe->jqhe', rounded.astype(jnp.float32), value_block)
        return output.reshape(width, heads * head_size)
    return lax.map(one_row, jnp.arange(rows_here, dtype=jnp.int32))

def layer(stream, gain, w_query, w_key, w_value, table):
    normed = normalize(stream, gain)
    query = jnp.dot(normed, w_query, preferred_element_type=jnp.float32).astype(jnp.bfloat16)
    keys = jnp.dot(normed, w_key, preferred_element_type=jnp.float32).astype(jnp.bfloat16)
    values = jnp.dot(normed, w_value, preferred_element_type=jnp.float32).astype(jnp.bfloat16)
    total_rows = stream.shape[0] // GRID_W
    shape = (total_rows, GRID_W, HEADS, HEAD_DIM)
    padding = ((4, 4), (0, 0), (0, 0), (0, 0))
    keys = jnp.pad(keys.reshape(shape), padding)
    values = jnp.pad(values.reshape(shape), padding)
    output = attend(query.reshape(shape), keys, values, table, 0, total_rows)
    return (stream.astype(jnp.float32) + output.reshape(stream.shape)).astype(jnp.bfloat16)

def reference(stream, gain_first, query_first, key_first, value_first, offset_first, gain_second, query_second, key_second, value_second, offset_second):
    middle = layer(stream, gain_first, query_first, key_first, value_first, offset_first)
    return layer(middle, gain_second, query_second, key_second, value_second, offset_second)
```

```python
import functools

import jax
import jax.numpy as jnp
from jax import lax
from jax.experimental import pallas as pl
from jax.experimental.pallas import tpu as pltpu
from jax.sharding import PartitionSpec as P

GRID_W = 64
HEAD = 128
ROWS = 8
TOK = ROWS * GRID_W
HALF = TOK // 2
PAD = 16
SIDE = 4
EPS = 1e-6
BLOCK = 2 * HEAD
LOW = 4 * GRID_W
HIGH = 3 * GRID_W
X, Y = 0, 1
LINKS = ((X, 1), (X, -1), (Y, 1), (Y, -1))
MESH_ID = pl.DeviceIdType.MESH


def weight_messages(axis, sign):
    part = 0 if sign > 0 else 1
    half = 1 if axis == X else 0
    own_first = 0 if axis == X else 2
    return (
        ("0a", (0, 0), own_first, 2),
        ("0b", (0, 0), 2 - own_first, 2),
        ("1a", (0, -1), 2 * half, 2),
        ("1a", (0, 1), 2 * half, 2),
        ("1a", (-sign, 0), own_first + part, 1),
        ("1b", (-sign, 0), 2 - own_first + part, 1),
        ("2a", (0, 2), 2 * half, 2),
        ("2b", (-sign, -1), 2 * half + part, 1),
        ("2b", (-sign, 1), 2 * half + part, 1),
        ("3", (-sign, 2), 2 * half + part, 1),
    )


SEND_AT = {
    (0, 0): (("send", 0, "0a"), ("send", 0, "0b")),
    (0, 1): (("wait", 0, "0a"), ("send", 0, "1a")),
    (0, 2): (("wait", 0, "0b"), ("send", 0, "1b")),
    (0, 4): (("wait", 0, "1a"), ("send", 0, "2a"), ("send", 0, "2b")),
    (0, 6): (("wait", 0, "2a"), ("send", 0, "3"), ("send", 1, "0a"), ("send", 1, "0b")),
    (0, 7): (("wait", 0, "1b"), ("wait", 0, "2b"), ("wait", 0, "3")),
    (1, 0): (("wait", 1, "0a"), ("wait", 1, "0b"), ("send", 1, "1a"), ("send", 1, "1b")),
    (1, 3): (("wait", 1, "1a"), ("wait", 1, "1b"), ("send", 1, "2a"), ("send", 1, "2b")),
    (1, 5): (("wait", 1, "2a"), ("send", 1, "3")),
    (1, 6): (("wait", 1, "2b"), ("wait", 1, "3")),
}


def kernel(
    zn,
    x_hbm,
    gains_hbm,
    q0_hbm,
    k0_hbm,
    v0_hbm,
    q1_hbm,
    k1_hbm,
    v1_hbm,
    table0,
    table1,
    out,
    xg,
    weights,
    kv,
    query,
    acc,
    square,
    tab,
    bias,
    local_sem,
    z_send,
    z_recv,
    core_send,
    core_recv,
    w_send,
    w_recv,
    halo_send,
    halo_recv,
):
    sp = lax.axis_index("sp")
    tp = lax.axis_index("tp")
    n_sp = SIDE * SIDE
    gx, gy = lax.rem(sp, SIDE), lax.div(sp, SIDE)
    core, z = lax.rem(tp, 2), lax.div(tp, 2)
    steps = zn // 2
    shards = n_sp // zn
    features = zn * BLOCK

    def at_z(offset):
        return lax.rem(z + offset + zn, zn)

    def chip(z_at, core_at):
        return {"sp": sp, "tp": z_at * 2 + core_at}

    def grid_sp(dx, dy):
        return lax.rem(gy + dy + SIDE, SIDE) * SIDE + lax.rem(gx + dx + SIDE, SIDE)

    def around(axis, along, across):
        along, across = (along + SIDE) % SIDE, (across + SIDE) % SIDE
        return grid_sp(along, across) if axis == X else grid_sp(across, along)

    sibling = chip(z, 1 - core)
    z_next, z_prev = chip(at_z(1), core), chip(at_z(-1), core)
    sp_next = {"sp": lax.rem(sp + 1, n_sp), "tp": tp}
    sp_prev = {"sp": lax.rem(sp + n_sp - 1, n_sp), "tp": tp}

    own = xg.at[0, z, core]
    loads = [
        pltpu.make_async_copy(x_hbm, own.at[0:TOK], local_sem.at[0]),
        pltpu.make_async_copy(gains_hbm, own.at[TOK : TOK + PAD], local_sem.at[1]),
    ]
    for layer, refs in enumerate(((q0_hbm, k0_hbm, v0_hbm), (q1_hbm, k1_hbm, v1_hbm))):
        for m, ref in enumerate(refs):
            loads.append(
                pltpu.make_async_copy(
                    ref, weights.at[layer, sp, :, m], local_sem.at[2 + 3 * layer + m]
                )
            )
    for load in loads:
        load.start()

    barrier = pltpu.get_barrier_semaphore()
    peers = [z_next, z_prev, sibling, sp_next, sp_prev]
    peers += [{"sp": around(axis, sign, 0), "tp": tp} for axis, sign in LINKS]
    for peer in peers:
        pl.semaphore_signal(barrier, inc=1, device_id=peer, device_id_type=MESH_ID)

    lanes = lax.broadcasted_iota(jnp.int32, (GRID_W, HEAD), 1) & (GRID_W - 1)
    column = lax.broadcasted_iota(jnp.int32, (GRID_W, HEAD), 0)
    first_column = jnp.clip(column - 8, 0, GRID_W - 16)
    in_window = (lanes >= first_column) & (lanes < first_column + 16)
    for layer, table in enumerate((table0, table1)):
        tab[...] = jnp.zeros_like(tab)
        tab[0:15, 0:31] = table[0]
        rows = tab[...]
        both = rows + pltpu.roll(pltpu.roll(rows, 15, 0), GRID_W, 1)
        for offset in range(14):
            spread = jnp.broadcast_to(both[offset : offset + 1], (GRID_W, HEAD))
            band = pltpu.roll(spread, HEAD - 15, 1, stride=1, stride_axis=0)
            bias[layer, offset] = jnp.where(in_window, band, -1e30)

    pl.semaphore_wait(barrier, len(peers))

    def remote(src, dst, send_sem, recv_sem, device):
        return pltpu.make_async_remote_copy(
            src_ref=src,
            dst_ref=dst,
            send_sem=send_sem,
            recv_sem=recv_sem,
            device_id=device,
            device_id_type=MESH_ID,
        )

    def chunk_rows(layer, chunk):
        if chunk == 0:
            return pl.ds(0, HALF)
        return pl.ds(HALF, HALF + (PAD if layer == 0 else 0))

    def z_copy(layer, origin, chunk, direction, step):
        ref = xg.at[layer, origin, core, chunk_rows(layer, chunk)]
        return remote(
            ref,
            ref,
            z_send.at[layer],
            z_recv.at[layer, direction, step, chunk],
            z_next if direction == 0 else z_prev,
        )

    def core_copy(layer, origin, chunk, from_core):
        ref = xg.at[layer, origin, from_core, chunk_rows(layer, chunk)]
        return remote(ref, ref, core_send.at[layer], core_recv.at[layer, origin, chunk], sibling)

    def weight_copy(layer, link, index, inbound):
        axis, sign = LINKS[link]
        _, (along, across), piece, pieces = weight_messages(axis, sign)[index]
        origin = around(axis, along - (sign if inbound else 0), across)
        ref = weights.at[layer, origin, pl.ds(piece, pieces)]
        return remote(
            ref,
            ref,
            w_send.at[layer],
            w_recv.at[layer, link, index],
            {"sp": around(axis, sign, 0), "tp": tp},
        )

    def weight_round(action, layer, name):
        for index in range(10):
            for link, (axis, sign) in enumerate(LINKS):
                if weight_messages(axis, sign)[index][0] == name:
                    copy = weight_copy(layer, link, index, action == "wait")
                    if action == "wait":
                        copy.wait_recv()
                    else:
                        copy.start()

    def add_block(layer, origin):
        for chunk in range(2):
            core_copy(layer, origin, chunk, 1 - core).wait_recv()
        columns = []
        for m in range(3):
            pieces = weights[layer, pl.ds(origin * shards, shards), :, m]
            columns.append(pieces.reshape(BLOCK, HEAD))
        right = jnp.concatenate(columns, axis=1)
        gains = [
            xg[0, origin, c, TOK : TOK + PAD, :].astype(jnp.float32)[layer : layer + 1]
            for c in range(2)
        ]
        for top in range(0, TOK, 128):
            rows = slice(top, top + 128)
            scaled, squares = [], square[rows, :]
            for c in range(2):
                wide = xg[layer, origin, c, rows, :].astype(jnp.float32)
                squares = squares + wide * wide
                scaled.append((wide * gains[c]).astype(jnp.bfloat16))
            square[rows, :] = squares
            acc[rows, :] += jnp.dot(
                jnp.concatenate(scaled, axis=1), right, preferred_element_type=jnp.float32
            )

    def blocks_between(layer, low, high):
        @pl.loop(low, high)
        def _(offset):
            add_block(layer, at_z(offset))

    def gather_step(layer, step):
        last = step == steps
        for chunk in range(2):
            for direction in range(2):
                if last and chunk != direction:
                    continue
                origin = at_z(-step if direction == 0 else step)
                if step > 0:
                    z_copy(layer, origin, chunk, direction, step - 1).wait_recv()
                if step < steps - 1 or (step == steps - 1 and chunk == direction):
                    z_copy(layer, origin, chunk, direction, step).start()
                if step > 0 or direction == 0:
                    core_copy(layer, origin, chunk, core).start()

    def project(layer):
        mean = jnp.sum(square[...], axis=1, keepdims=True) * (1.0 / features)
        scale = lax.rsqrt(mean + EPS)
        kv[layer, LOW : LOW + TOK, :] = (acc[:, HEAD:] * scale).astype(jnp.bfloat16)
        query[...] = (acc[:, :HEAD] * scale).astype(jnp.bfloat16)

    def halo_copies(layer):
        up = remote(
            kv.at[layer, pl.ds(TOK, LOW)],
            kv.at[layer, pl.ds(0, LOW)],
            halo_send.at[layer, 0],
            halo_recv.at[layer, 0],
            sp_next,
        )
        down = remote(
            kv.at[layer, pl.ds(LOW, HIGH)],
            kv.at[layer, pl.ds(LOW + TOK, HIGH)],
            halo_send.at[layer, 1],
            halo_recv.at[layer, 1],
            sp_prev,
        )
        return up, down

    def attend(layer, row):
        grid_row = sp * ROWS + row
        first = jnp.clip(grid_row - 4, 0, n_sp * ROWS - 8)
        start = pl.multiple_of((first - sp * ROWS + 4) * GRID_W, GRID_W)
        offset = first - grid_row + 7
        window = pl.ds(start, 8 * GRID_W)
        score = lax.dot_general(
            query[row * GRID_W : (row + 1) * GRID_W, :],
            kv[layer, window, 0:HEAD],
            (((1,), (1,)), ((), ())),
            preferred_element_type=jnp.float32,
        )
        bands = jnp.concatenate([bias[layer, offset + 2 * m] for m in range(4)], axis=1)
        score = score * (HEAD**-0.5) + bands
        weight = jnp.exp(score - jnp.max(score, axis=1, keepdims=True))
        total = jnp.sum(weight, axis=1, keepdims=True)
        mixed = jnp.dot(
            weight.astype(jnp.bfloat16), kv[layer, window, HEAD:], preferred_element_type=jnp.float32
        )
        return mixed / total

    loads[0].wait()
    loads[1].wait()
    for layer in range(2):
        acc[...] = jnp.zeros_like(acc)
        square[...] = jnp.zeros_like(square)
        for step in range(steps + 1):
            if layer == 0 or step > 0:
                gather_step(layer, step)
            if layer == 0 and step == 0:
                for load in loads[2:]:
                    load.wait()
            for at in range(8):
                if at == step or (step == steps and at > step):
                    for action, which, name in SEND_AT.get((layer, at), ()):
                        weight_round(action, which, name)
            if step == max(steps - 1, 1):
                blocks_between(layer, 1 - steps, steps)
        add_block(layer, at_z(steps))
        project(layer)
        up, down = halo_copies(layer)
        up.start()
        down.start()
        up.wait_recv()
        down.wait_recv()
        for chunk in range(2):
            for row in range(4 * chunk, 4 * chunk + 4):
                rows = slice(row * GRID_W, (row + 1) * GRID_W)
                x = xg[layer, z, core, rows, :].astype(jnp.float32)
                result = (x + attend(layer, row)).astype(jnp.bfloat16)
                if layer == 0:
                    xg[1, z, core, rows, :] = result
                else:
                    out[rows, :] = result
            if layer == 0:
                for direction in range(2):
                    if steps > 1 or chunk == direction:
                        z_copy(1, z, chunk, direction, 0).start()
                core_copy(1, z, chunk, core).start()

    for layer in range(2):
        rows = pl.ds(0, TOK + (PAD if layer == 0 else 0))
        sent = xg.at[layer, pl.ds(0, zn - 1), 0, rows]
        remote(sent, sent, z_send.at[layer], z_recv.at[layer, 0, 0, 0], z_next).wait_send()
        sent = xg.at[layer, pl.ds(0, zn), 0, rows]
        remote(sent, sent, core_send.at[layer], core_recv.at[layer, 0, 0], sibling).wait_send()
        sent = weights.at[layer, pl.ds(0, n_sp - 1)]
        remote(sent, sent, w_send.at[layer], w_recv.at[layer, 0, 0], sp_next).wait_send()
        for copy in halo_copies(layer):
            copy.wait_send()


def body(zn, x, gain0, q0, k0, v0, table0, gain1, q1, k1, v1, table1):
    gains = jnp.pad(jnp.stack([gain0, gain1]), ((0, PAD - 2), (0, 0)))
    piece = q0.shape[0] // 4
    pieces = [w.reshape(4, piece, HEAD) for w in (q0, k0, v0, q1, k1, v1)]
    steps = zn // 2
    n_sp = SIDE * SIDE
    hbm = pl.BlockSpec(memory_space=pltpu.HBM)
    vmem = pl.BlockSpec(memory_space=pltpu.VMEM)
    dma = pltpu.SemaphoreType.DMA
    return pl.pallas_call(
        functools.partial(kernel, zn),
        out_shape=jax.ShapeDtypeStruct((TOK, HEAD), jnp.bfloat16),
        in_specs=[hbm] * 8 + [vmem] * 2,
        out_specs=vmem,
        scratch_shapes=[
            pltpu.VMEM((2, zn, 2, TOK + PAD, HEAD), jnp.bfloat16),
            pltpu.VMEM((2, n_sp, 4, 3, piece, HEAD), jnp.bfloat16),
            pltpu.VMEM((2, LOW + TOK + 4 * GRID_W, 2 * HEAD), jnp.bfloat16),
            pltpu.VMEM((TOK, HEAD), jnp.bfloat16),
            pltpu.VMEM((TOK, 3 * HEAD), jnp.float32),
            pltpu.VMEM((TOK, HEAD), jnp.float32),
            pltpu.VMEM((16, HEAD), jnp.float32),
            pltpu.VMEM((2, 14, GRID_W, HEAD), jnp.float32),
            dma((8,)),
            dma((2,)),
            dma((2, 2, steps, 2)),
            dma((2,)),
            dma((2, zn, 2)),
            dma((2,)),
            dma((2, 4, 10)),
            dma((2, 2)),
            dma((2, 2)),
        ],
        compiler_params=pltpu.CompilerParams(
            collective_id=0, has_side_effects=True, vmem_limit_bytes=48 * 1024 * 1024
        ),
        name="neighbourhood",
    )(x, gains, *pieces, table0, table1)


def solution(mesh):
    placed = (
        P("sp", "tp"),
        P("tp"),
        P("sp", "tp"),
        P("sp", "tp"),
        P("sp", "tp"),
        P("tp", None, None),
        P("tp"),
        P("sp", "tp"),
        P("sp", "tp"),
        P("sp", "tp"),
        P("tp", None, None),
    )
    return jax.shard_map(
        functools.partial(body, mesh.shape["tp"] // 2),
        mesh=mesh,
        in_specs=placed,
        out_specs=P("sp", "tp"),
        check_vma=False,
    )
```

```python
import functools

import jax
import jax.numpy as jnp
from jax import lax
from jax.experimental import pallas as pl
from jax.experimental.pallas import tpu as pltpu
from jax.sharding import PartitionSpec as P

GRID_W = 64
HEAD = 128
ROWS = 8
TOK = ROWS * GRID_W
CHUNKS = 4
PART = TOK // CHUNKS
PAD = 16
SIDE = 4
EPS = 1e-6
BLOCK = 2 * HEAD
LOW = 4 * GRID_W
HIGH = 3 * GRID_W
X, Y = 0, 1
LINKS = ((X, 1), (X, -1), (Y, 1), (Y, -1))
MESH_ID = pl.DeviceIdType.MESH


def weight_messages(axis, sign):
    part = 0 if sign > 0 else 1
    half = 1 if axis == X else 0
    own_first = 0 if axis == X else 2
    return (
        ("0a", (0, 0), own_first, 2),
        ("0b", (0, 0), 2 - own_first, 2),
        ("1a", (0, -1), 2 * half, 2),
        ("1a", (0, 1), 2 * half, 2),
        ("1a", (-sign, 0), own_first + part, 1),
        ("1b", (-sign, 0), 2 - own_first + part, 1),
        ("2a", (0, 2), 2 * half, 2),
        ("2b", (-sign, -1), 2 * half + part, 1),
        ("2b", (-sign, 1), 2 * half + part, 1),
        ("3", (-sign, 2), 2 * half + part, 1),
    )


WEIGHTS_AT = {
    (0, 0): (("send", 0, "0a"), ("send", 0, "0b")),
    (0, 1): (("wait", 0, "0a"), ("send", 0, "1a")),
    (0, 2): (("wait", 0, "0b"), ("send", 0, "1b")),
    (0, 3): (("wait", 0, "1a"), ("send", 0, "2a"), ("send", 0, "2b")),
    (0, 5): (("wait", 0, "2a"), ("send", 0, "3"), ("send", 1, "0a"), ("send", 1, "0b")),
    (0, 6): (("wait", 0, "1b"), ("wait", 0, "2b"), ("wait", 0, "3")),
    (0, "halo"): (("wait", 1, "0a"), ("wait", 1, "0b"), ("send", 1, "1a"), ("send", 1, "1b")),
    (1, 2): (("wait", 1, "1a"), ("wait", 1, "1b"), ("send", 1, "2a"), ("send", 1, "2b")),
    (1, 4): (("wait", 1, "2a"), ("send", 1, "3")),
    (1, 5): (("wait", 1, "2b"), ("wait", 1, "3")),
}
BLOCKS_AT = {
    (0, 7): (range(-6, -2), range(-2, 2), range(2, 7)),
    (0, 8): ((-7, 7),),
    (1, 6): (range(-5, -1), range(-1, 2), range(2, 6)),
    (1, 7): ((-6, 6),),
    (1, 8): ((-7, 7),),
}
MASKED = -1e30


def kernel(
    zn,
    x_hbm,
    gain0_hbm,
    gain1_hbm,
    q0_hbm,
    k0_hbm,
    v0_hbm,
    q1_hbm,
    k1_hbm,
    v1_hbm,
    table0_hbm,
    table1_hbm,
    out,
    xg,
    weights,
    kv,
    query,
    acc,
    square,
    own_gains,
    gains,
    tables,
    tab,
    band,
    own_bias,
    low_bias,
    high_bias,
    local_sem,
    z_send,
    z_recv,
    core_send,
    core_recv,
    gain_send,
    gain_recv,
    gain_core_send,
    gain_core_recv,
    w_send,
    w_recv,
    halo_send,
    halo_recv,
):
    sp = lax.axis_index("sp")
    tp = lax.axis_index("tp")
    n_sp = SIDE * SIDE
    gx, gy = lax.rem(sp, SIDE), lax.div(sp, SIDE)
    core, z = lax.rem(tp, 2), lax.div(tp, 2)
    steps = zn // 2
    shards = n_sp // zn
    features = zn * BLOCK

    def at_z(offset):
        return lax.rem(z + offset + zn, zn)

    def chip(z_at, core_at):
        return {"sp": sp, "tp": z_at * 2 + core_at}

    def grid_sp(dx, dy):
        return lax.rem(gy + dy + SIDE, SIDE) * SIDE + lax.rem(gx + dx + SIDE, SIDE)

    def around(axis, along, across):
        along, across = (along + SIDE) % SIDE, (across + SIDE) % SIDE
        return grid_sp(along, across) if axis == X else grid_sp(across, along)

    sibling = chip(z, 1 - core)
    z_next, z_prev = chip(at_z(1), core), chip(at_z(-1), core)
    sp_next = {"sp": lax.rem(sp + 1, n_sp), "tp": tp}
    sp_prev = {"sp": lax.rem(sp + n_sp - 1, n_sp), "tp": tp}

    loads = [
        pltpu.make_async_copy(x_hbm, xg.at[0, z, core], local_sem.at[0]),
        pltpu.make_async_copy(gain0_hbm, own_gains.at[0], local_sem.at[1]),
        pltpu.make_async_copy(gain1_hbm, own_gains.at[1], local_sem.at[2]),
        pltpu.make_async_copy(table0_hbm, tables.at[0], local_sem.at[3]),
        pltpu.make_async_copy(table1_hbm, tables.at[1], local_sem.at[4]),
    ]
    for layer, refs in enumerate(((q0_hbm, k0_hbm, v0_hbm), (q1_hbm, k1_hbm, v1_hbm))):
        for m, ref in enumerate(refs):
            loads.append(
                pltpu.make_async_copy(
                    ref, weights.at[layer, sp, :, m], local_sem.at[5 + 3 * layer + m]
                )
            )
    for load in loads:
        load.start()

    barrier = pltpu.get_barrier_semaphore()
    peers = [z_next, z_prev, sibling, sp_next, sp_prev]
    peers += [{"sp": around(axis, sign, 0), "tp": tp} for axis, sign in LINKS]
    for peer in peers:
        pl.semaphore_signal(barrier, inc=1, device_id=peer, device_id_type=MESH_ID)

    loads[1].wait()
    loads[2].wait()
    spare = jnp.zeros((PAD - 2, HEAD), jnp.float32)
    both_gains = [own_gains[layer].astype(jnp.float32) for layer in range(2)]
    gains[z, core] = jnp.concatenate(both_gains + [spare]).astype(jnp.bfloat16)
    for layer in range(2):
        kv[layer, LOW + TOK + HIGH :, :] = jnp.zeros((GRID_W, 2 * HEAD), jnp.bfloat16)

    def build_bias(layer):
        lanes = lax.broadcasted_iota(jnp.int32, (GRID_W, HEAD), 1)
        key_column = lanes & (GRID_W - 1)
        column = lax.broadcasted_iota(jnp.int32, (GRID_W, HEAD), 0)
        first_column = jnp.clip(column - 8, 0, GRID_W - 16)
        in_window = (key_column >= first_column) & (key_column < first_column + 16)
        tab[...] = jnp.zeros_like(tab)
        tab[0:15, 0:31] = tables[layer, :, 0, :]
        rows = tab[...]
        both = rows + pltpu.roll(pltpu.roll(rows, 15, 0), GRID_W, 1)
        for offset in range(14):
            spread = jnp.broadcast_to(both[offset : offset + 1], (GRID_W, HEAD))
            shifted = pltpu.roll(spread, HEAD - 15, 1, stride=1, stride_axis=0)
            band[offset] = jnp.where(in_window, shifted, MASKED)
        at_start = jnp.where(sp == 0, 0.0, MASKED)
        at_end = jnp.where(sp == n_sp - 1, 0.0, MASKED)
        not_start = jnp.where(sp == 0, MASKED, 0.0)
        not_end = jnp.where(sp == n_sp - 1, MASKED, 0.0)
        right = lanes >= GRID_W

        def pair(row, key_row, penalties):
            if penalties == (None, None):
                return jnp.full((GRID_W, HEAD), MASKED, jnp.float32)
            values = [MASKED if p is None else p for p in penalties]
            offset = key_row - row + 7
            base = band[offset]
            return base + jnp.where(right, values[1], values[0])

        def inside(row, key_row):
            return row - 4 <= key_row <= row + 3

        for row in range(ROWS):
            for m in range(0, ROWS, 2):
                penalties = tuple(
                    0.0 if inside(row, m + d) else (at_start if row < 4 else at_end)
                    for d in range(2)
                )
                own_bias[layer, row, :, m * GRID_W : (m + 2) * GRID_W] = pair(row, m, penalties)
            for m in range(0, 4, 2):
                lanes_at = slice(m * GRID_W, (m + 2) * GRID_W)
                if row < 4:
                    penalties = tuple(
                        not_start if inside(row, m + d - 4) else None for d in range(2)
                    )
                    low_bias[layer, row, :, lanes_at] = pair(row, m - 4, penalties)
                else:
                    penalties = tuple(not_end if inside(row, m + d + 8) else None for d in range(2))
                    high_bias[layer, row - 4, :, lanes_at] = pair(row, m + 8, penalties)

    pl.semaphore_wait(barrier, len(peers))

    def remote(src, dst, send_sem, recv_sem, device):
        return pltpu.make_async_remote_copy(
            src_ref=src,
            dst_ref=dst,
            send_sem=send_sem,
            recv_sem=recv_sem,
            device_id=device,
            device_id_type=MESH_ID,
        )

    def chunk_rows(chunk):
        start = chunk * PART
        return pl.ds(start if isinstance(chunk, int) else pl.multiple_of(start, PART), PART)

    def z_copy(layer, origin, chunk, direction, step):
        ref = xg.at[layer, origin, core, chunk_rows(chunk)]
        return remote(
            ref,
            ref,
            z_send.at[layer],
            z_recv.at[layer, direction, step, chunk],
            z_next if direction == 0 else z_prev,
        )

    def core_copy(layer, origin, chunk, from_core):
        ref = xg.at[layer, origin, from_core, chunk_rows(chunk)]
        return remote(ref, ref, core_send.at[layer], core_recv.at[layer, origin, chunk], sibling)

    def gain_copy(origin, direction, step):
        ref = gains.at[origin, core]
        device = z_next if direction == 0 else z_prev
        return remote(ref, ref, gain_send, gain_recv.at[direction, step], device)

    def gain_core_copy(origin, from_core):
        ref = gains.at[origin, from_core]
        return remote(ref, ref, gain_core_send, gain_core_recv.at[origin], sibling)

    def weight_copy(layer, link, index, inbound):
        axis, sign = LINKS[link]
        _, (along, across), piece, pieces = weight_messages(axis, sign)[index]
        origin = around(axis, along - (sign if inbound else 0), across)
        ref = weights.at[layer, origin, pl.ds(piece, pieces)]
        return remote(
            ref,
            ref,
            w_send.at[layer],
            w_recv.at[layer, link, index],
            {"sp": around(axis, sign, 0), "tp": tp},
        )

    def weight_round(action, layer, name):
        for index in range(10):
            for link, (axis, sign) in enumerate(LINKS):
                if weight_messages(axis, sign)[index][0] == name:
                    copy = weight_copy(layer, link, index, action == "wait")
                    if action == "wait":
                        copy.wait_recv()
                    else:
                        copy.start()

    def add_rows(layer, offsets, chunk):
        rows = chunk_rows(chunk)
        origins = [at_z(offset) for offset in offsets]
        for origin in origins:
            core_copy(layer, origin, chunk, 1 - core).wait_recv()
        squares, scaled, right = square[rows, :], [], []
        for origin in origins:
            for c in range(2):
                wide = xg[layer, origin, c, rows, :].astype(jnp.float32)
                gain = gains[origin, c].astype(jnp.float32)[layer : layer + 1]
                squares = squares + wide * wide
                scaled.append((wide * gain).astype(jnp.bfloat16))
            columns = []
            for m in range(3):
                pieces = weights[layer, pl.ds(origin * shards, shards), :, m]
                columns.append(pieces.reshape(BLOCK, HEAD))
            right.append(jnp.concatenate(columns, axis=1))
        square[rows, :] = squares
        acc[rows, :] += jnp.dot(
            jnp.concatenate(scaled, axis=1),
            jnp.concatenate(right, axis=0),
            preferred_element_type=jnp.float32,
        )

    def await_gains(offsets):
        for offset in offsets:
            gain_core_copy(at_z(offset), 1 - core).wait_recv()

    def gather_step(layer, step):
        origins = (at_z(-step), at_z(step))
        if layer == 0:
            for direction in range(2):
                if step == steps and direction == 1:
                    continue
                if step > 0:
                    gain_copy(origins[direction], direction, step - 1).wait_recv()
                if step < steps - 1 or (step == steps - 1 and direction == 0):
                    gain_copy(origins[direction], direction, step).start()
                if step > 0 or direction == 0:
                    gain_core_copy(origins[direction], core).start()
        groups = BLOCKS_AT.get((layer, step), ())
        if layer == 0:
            await_gains([offset for group in groups for offset in group])
        for far in (True, False):

            @pl.loop(0 if far else CHUNKS // 2, CHUNKS // 2 if far else CHUNKS)
            def _(slot):
                for direction in range(2):
                    if step == steps and not far:
                        continue
                    chunk = slot if direction == 0 else lax.rem(slot + CHUNKS // 2, CHUNKS)
                    if step > 0:
                        z_copy(layer, origins[direction], chunk, direction, step - 1).wait_recv()
                    if step < steps - 1 or (step == steps - 1 and far):
                        z_copy(layer, origins[direction], chunk, direction, step).start()
                    if step > 0 or direction == 0:
                        core_copy(layer, origins[direction], chunk, core).start()
                for offsets in groups:
                    add_rows(layer, offsets, slot)

    def project(layer):
        mean = jnp.sum(square[...], axis=1, keepdims=True) * (1.0 / features)
        scale = lax.rsqrt(mean + EPS)
        kv[layer, LOW : LOW + TOK, :] = (acc[:, HEAD:] * scale).astype(jnp.bfloat16)
        up, down = halo_copies(layer)
        up.start()
        down.start()
        query[...] = (acc[:, :HEAD] * scale).astype(jnp.bfloat16)

    def halo_copies(layer):
        up = remote(
            kv.at[layer, pl.ds(TOK, LOW)],
            kv.at[layer, pl.ds(0, LOW)],
            halo_send.at[layer, 0],
            halo_recv.at[layer, 0],
            sp_next,
        )
        down = remote(
            kv.at[layer, pl.ds(LOW, HIGH)],
            kv.at[layer, pl.ds(LOW + TOK, HIGH)],
            halo_send.at[layer, 1],
            halo_recv.at[layer, 1],
            sp_prev,
        )
        return up, down

    def scores(layer, chunk, keys, bias, first_row):
        score = lax.dot_general(
            query[chunk_rows(chunk), :],
            kv[layer, keys, 0:HEAD],
            (((1,), (1,)), ((), ())),
            preferred_element_type=jnp.float32,
        )
        grid_rows = PART // GRID_W
        start = chunk * grid_rows - first_row
        band_of = [bias[layer, start + i] for i in range(grid_rows)]
        return score * (HEAD**-0.5) + jnp.concatenate(band_of, axis=0)

    def mix(layer, weight, keys):
        return jnp.dot(
            weight.astype(jnp.bfloat16), kv[layer, keys, HEAD:], preferred_element_type=jnp.float32
        )

    def attend_own(layer, chunk):
        keys = pl.ds(LOW, TOK)
        score = scores(layer, chunk, keys, own_bias, 0)
        most = jnp.max(score, axis=1, keepdims=True)
        weight = jnp.exp(score - most)
        return most, jnp.sum(weight, axis=1, keepdims=True), mix(layer, weight, keys)

    def attend_halo(layer, chunk, own_part):
        most, total, mixed = own_part
        low = chunk < CHUNKS // 2
        keys = pl.ds(0 if low else LOW + TOK, LOW)
        bias, first_row = (low_bias, 0) if low else (high_bias, 4)
        score = scores(layer, chunk, keys, bias, first_row)
        over = jnp.maximum(most, jnp.max(score, axis=1, keepdims=True))
        weight = jnp.exp(score - over)
        kept = jnp.exp(most - over)
        total = total * kept + jnp.sum(weight, axis=1, keepdims=True)
        return (mixed * kept + mix(layer, weight, keys)) / total

    def weight_rounds(layer, at):
        for action, which, name in WEIGHTS_AT.get((layer, at), ()):
            weight_round(action, which, name)

    loads[0].wait()
    for layer in range(2):
        for step in range(steps + 1):
            if layer == 0 or step > 0:
                gather_step(layer, step)
            if layer == 0 and step == 0:
                for load in loads[5:]:
                    load.wait()
            weight_rounds(layer, step)
            if layer == 0 and step == 0:
                for at in range(2):
                    loads[3 + at].wait()
                    build_bias(at)
            if step == 0:
                acc[...] = jnp.zeros_like(acc)
                square[...] = jnp.zeros_like(square)

        if layer == 0:
            await_gains((steps,))

        @pl.loop(0, CHUNKS)
        def _(chunk):
            add_rows(layer, (steps,), chunk)

        project(layer)
        weight_rounds(layer, "halo")
        own_parts = [attend_own(layer, chunk) for chunk in range(CHUNKS)]
        up, down = halo_copies(layer)
        for chunk in range(CHUNKS):
            if chunk == 0:
                up.wait_recv()
            if chunk == CHUNKS // 2:
                down.wait_recv()
            rows = chunk_rows(chunk)
            x = xg[layer, z, core, rows, :].astype(jnp.float32)
            result = (x + attend_halo(layer, chunk, own_parts[chunk])).astype(jnp.bfloat16)
            if layer == 0:
                xg[1, z, core, rows, :] = result
                for direction in range(2):
                    z_copy(1, z, chunk, direction, 0).start()
                core_copy(1, z, chunk, core).start()
            else:
                out[rows, :] = result

    sent = gains.at[pl.ds(0, zn - 1), 0]
    remote(sent, sent, gain_send, gain_recv.at[0, 0], z_next).wait_send()
    sent = gains.at[pl.ds(0, zn), 0]
    remote(sent, sent, gain_core_send, gain_core_recv.at[0], sibling).wait_send()
    for layer in range(2):
        sent = xg.at[layer, pl.ds(0, zn - 1), 0]
        remote(sent, sent, z_send.at[layer], z_recv.at[layer, 0, 0, 0], z_next).wait_send()
        sent = xg.at[layer, pl.ds(0, zn), 0]
        remote(sent, sent, core_send.at[layer], core_recv.at[layer, 0, 0], sibling).wait_send()
        sent = weights.at[layer, pl.ds(0, n_sp - 1)]
        remote(sent, sent, w_send.at[layer], w_recv.at[layer, 0, 0], sp_next).wait_send()
        for copy in halo_copies(layer):
            copy.wait_send()


def body(zn, x, gain0, q0, k0, v0, table0, gain1, q1, k1, v1, table1):
    piece = q0.shape[0] // 4
    pieces = [w.reshape(4, piece, HEAD) for w in (q0, k0, v0, q1, k1, v1)]
    steps = zn // 2
    n_sp = SIDE * SIDE
    hbm = pl.BlockSpec(memory_space=pltpu.HBM)
    vmem = pl.BlockSpec(memory_space=pltpu.VMEM)
    dma = pltpu.SemaphoreType.DMA
    return pl.pallas_call(
        functools.partial(kernel, zn),
        out_shape=jax.ShapeDtypeStruct((TOK, HEAD), jnp.bfloat16),
        in_specs=[hbm] * 11,
        out_specs=vmem,
        scratch_shapes=[
            pltpu.VMEM((2, zn, 2, TOK, HEAD), jnp.bfloat16),
            pltpu.VMEM((2, n_sp, 4, 3, piece, HEAD), jnp.bfloat16),
            pltpu.VMEM((2, LOW + TOK + 4 * GRID_W, 2 * HEAD), jnp.bfloat16),
            pltpu.VMEM((TOK, HEAD), jnp.bfloat16),
            pltpu.VMEM((TOK, 3 * HEAD), jnp.float32),
            pltpu.VMEM((TOK, HEAD), jnp.float32),
            pltpu.VMEM((2, 1, HEAD), jnp.bfloat16),
            pltpu.VMEM((zn, 2, PAD, HEAD), jnp.bfloat16),
            pltpu.VMEM((2, 15, 1, 31), jnp.float32),
            pltpu.VMEM((16, HEAD), jnp.float32),
            pltpu.VMEM((14, GRID_W, HEAD), jnp.float32),
            pltpu.VMEM((2, ROWS, GRID_W, TOK), jnp.float32),
            pltpu.VMEM((2, 4, GRID_W, LOW), jnp.float32),
            pltpu.VMEM((2, 4, GRID_W, LOW), jnp.float32),
            dma((11,)),
            dma((2,)),
            dma((2, 2, steps, CHUNKS)),
            dma((2,)),
            dma((2, zn, CHUNKS)),
            dma,
            dma((2, steps)),
            dma,
            dma((zn,)),
            dma((2,)),
            dma((2, 4, 10)),
            dma((2, 2)),
            dma((2, 2)),
        ],
        compiler_params=pltpu.CompilerParams(
            collective_id=0, has_side_effects=True, vmem_limit_bytes=67043328
        ),
        name="neighbourhood",
    )(
        x,
        gain0.reshape(1, HEAD),
        gain1.reshape(1, HEAD),
        *pieces,
        jnp.swapaxes(table0, 0, 1),
        jnp.swapaxes(table1, 0, 1),
    )


def solution(mesh):
    placed = (
        P("sp", "tp"),
        P("tp"),
        P("sp", "tp"),
        P("sp", "tp"),
        P("sp", "tp"),
        P("tp", None, None),
        P("tp"),
        P("sp", "tp"),
        P("sp", "tp"),
        P("sp", "tp"),
        P("tp", None, None),
    )
    return jax.shard_map(
        functools.partial(body, mesh.shape["tp"] // 2),
        mesh=mesh,
        in_specs=placed,
        out_specs=P("sp", "tp"),
        check_vma=False,
    )
```

```python
import functools

import jax
import jax.numpy as jnp
from jax import lax
from jax.experimental import pallas as pl
from jax.experimental.pallas import tpu as pltpu
from jax.sharding import PartitionSpec as P

GRID_W = 64
HEAD = 128
ROWS = 8
TOK = ROWS * GRID_W
CHUNKS = 4
PART = TOK // CHUNKS
PAD = 16
SIDE = 4
EPS = 1e-6
BLOCK = 2 * HEAD
LOW = 4 * GRID_W
HIGH = 3 * GRID_W
X, Y = 0, 1
LINKS = ((X, 1), (X, -1), (Y, 1), (Y, -1))
MESH_ID = pl.DeviceIdType.MESH


def weight_messages(axis, sign):
    part = 0 if sign > 0 else 1
    half = 1 if axis == X else 0
    own_first = 0 if axis == X else 2
    return (
        ("0a", 0, (0, 0), own_first, 2),
        ("0b", 1, (0, 0), 2 - own_first, 2),
        ("1h", 2, (0, -1), 2 * half, 2),
        ("1h", 2, (0, 1), 2 * half, 2),
        ("1s", 3, (-sign, 0), own_first + part, 1),
        ("1b", 4, (-sign, 0), 2 - own_first + part, 1),
        ("2a", 5, (0, 2), 2 * half, 2),
        ("2b", 6, (-sign, -1), 2 * half + part, 1),
        ("2b", 6, (-sign, 1), 2 * half + part, 1),
        ("3", 7, (-sign, 2), 2 * half + part, 1),
    )


WEIGHTS_AT = {
    (0, 0, 7): (("send", 0, "0a"), ("send", 0, "0b")),
    (0, 1, 3): (("wait", 0, "0a"), ("send", 0, "1s"), ("send", 0, "1h")),
    (0, 2, 6): (("wait", 0, "1s"), ("send", 0, "2a"), ("wait", 0, "0b"), ("send", 0, "1b")),
    (0, 4, 0): (("wait", 0, "1h"), ("send", 0, "2b")),
    (0, 4, 6): (("wait", 0, "2a"), ("send", 0, "3")),
    (0, 6, 2): (
        ("wait", 0, "1b"),
        ("wait", 0, "2b"),
        ("wait", 0, "3"),
        ("send", 1, "0a"),
        ("send", 1, "0b"),
    ),
    (0, 8, 2): (("wait", 1, "0a"), ("send", 1, "1s")),
    (0, "halo", 0): (
        ("wait", 1, "1s"),
        ("send", 1, "2a"),
        ("send", 1, "1h"),
        ("wait", 1, "0b"),
        ("send", 1, "1b"),
    ),
    (1, 1, 5): (("wait", 1, "2a"), ("send", 1, "3")),
    (1, 2, 4): (("wait", 1, "1h"), ("send", 1, "2b")),
    (1, 4, 0): (("wait", 1, "1b"), ("wait", 1, "2b"), ("wait", 1, "3")),
}
BLOCKS_AT = {
    (0, 6, 3): (0,),
    (0, 6, 4): (-1, 1),
    (0, 6, 6): (-2, 2),
    (0, 7, 1): (-3, 3),
    (0, 7, 3): (-4, 4),
    (0, 7, 5): (-5, 5),
    (0, 7, 7): (-6, 6),
    (0, 8, 2): (-7, 7),
    (1, 4, 2): (0,),
    (1, 4, 4): (-1, 1),
    (1, 4, 6): (-2, 2),
    (1, 5, 2): (-3, 3),
    (1, 5, 6): (-4, 4),
    (1, 6, 6): (-5, 5),
    (1, 7, 5): (-6, 6),
    (1, 8, 2): (-7, 7),
}
MASKED = -1e30


def kernel(
    zn,
    x_hbm,
    gain0_hbm,
    gain1_hbm,
    q0_hbm,
    k0_hbm,
    v0_hbm,
    q1_hbm,
    k1_hbm,
    v1_hbm,
    table0_hbm,
    table1_hbm,
    out,
    xg,
    weights,
    kv,
    query,
    acc,
    square,
    own_gains,
    gains,
    tables,
    tab,
    band,
    own_bias,
    low_bias,
    high_bias,
    local_sem,
    z_send,
    z_recv,
    core_send,
    core_recv,
    own_recv,
    gain_send,
    gain_recv,
    gain_core_send,
    gain_core_recv,
    w_send,
    w_recv,
    halo_send,
    halo_recv,
):
    sp = lax.axis_index("sp")
    tp = lax.axis_index("tp")
    n_sp = SIDE * SIDE
    gx, gy = lax.rem(sp, SIDE), lax.div(sp, SIDE)
    core, z = lax.rem(tp, 2), lax.div(tp, 2)
    steps = zn // 2
    shards = n_sp // zn
    features = zn * BLOCK

    def at_z(offset):
        return lax.rem(z + offset + zn, zn)

    def chip(z_at, core_at):
        return {"sp": sp, "tp": z_at * 2 + core_at}

    def grid_sp(dx, dy):
        return lax.rem(gy + dy + SIDE, SIDE) * SIDE + lax.rem(gx + dx + SIDE, SIDE)

    def around(axis, along, across):
        along, across = (along + SIDE) % SIDE, (across + SIDE) % SIDE
        return grid_sp(along, across) if axis == X else grid_sp(across, along)

    sibling = chip(z, 1 - core)
    way = 2 * core - 1
    z_onward, z_source = chip(at_z(-way), core), chip(at_z(way), core)
    sp_next = {"sp": lax.rem(sp + 1, n_sp), "tp": tp}
    sp_prev = {"sp": lax.rem(sp + n_sp - 1, n_sp), "tp": tp}

    loads = [
        pltpu.make_async_copy(x_hbm, xg.at[0, z, core], local_sem.at[0]),
        pltpu.make_async_copy(gain0_hbm, own_gains.at[0], local_sem.at[1]),
        pltpu.make_async_copy(gain1_hbm, own_gains.at[1], local_sem.at[2]),
        pltpu.make_async_copy(table0_hbm, tables.at[0], local_sem.at[3]),
        pltpu.make_async_copy(table1_hbm, tables.at[1], local_sem.at[4]),
    ]
    for layer, refs in enumerate(((q0_hbm, k0_hbm, v0_hbm), (q1_hbm, k1_hbm, v1_hbm))):
        for m, ref in enumerate(refs):
            loads.append(
                pltpu.make_async_copy(
                    ref, weights.at[layer, sp, :, m], local_sem.at[5 + 3 * layer + m]
                )
            )
    for load in loads:
        load.start()

    barrier = pltpu.get_barrier_semaphore()
    peers = [z_source, sibling, sp_next, sp_prev]
    peers += [{"sp": around(axis, sign, 0), "tp": tp} for axis, sign in LINKS]
    for peer in peers:
        pl.semaphore_signal(barrier, inc=1, device_id=peer, device_id_type=MESH_ID)

    for layer in range(2):
        kv[layer, :, LOW + TOK + HIGH :, :] = jnp.zeros((2, GRID_W, HEAD), jnp.bfloat16)

    def build_bias(layer):
        lanes = lax.broadcasted_iota(jnp.int32, (GRID_W, HEAD), 1)
        key_column = lanes & (GRID_W - 1)
        column = lax.broadcasted_iota(jnp.int32, (GRID_W, HEAD), 0)
        first_column = jnp.clip(column - 8, 0, GRID_W - 16)
        in_window = (key_column >= first_column) & (key_column < first_column + 16)
        tab[...] = jnp.zeros_like(tab)
        tab[0:15, 0:31] = tables[layer, :, 0, :]
        rows = tab[...]
        both = rows + pltpu.roll(pltpu.roll(rows, 15, 0), GRID_W, 1)
        for offset in range(14):
            spread = jnp.broadcast_to(both[offset : offset + 1], (GRID_W, HEAD))
            shifted = pltpu.roll(spread, HEAD - 15, 1, stride=1, stride_axis=0)
            band[offset] = jnp.where(in_window, shifted, MASKED)
        at_start = jnp.where(sp == 0, 0.0, MASKED)
        at_end = jnp.where(sp == n_sp - 1, 0.0, MASKED)
        not_start = jnp.where(sp == 0, MASKED, 0.0)
        not_end = jnp.where(sp == n_sp - 1, MASKED, 0.0)
        right = lanes >= GRID_W

        def pair(row, key_row, penalties):
            if penalties == (None, None):
                return jnp.full((GRID_W, HEAD), MASKED, jnp.float32)
            values = [MASKED if p is None else p for p in penalties]
            offset = key_row - row + 7
            base = band[offset]
            return base + jnp.where(right, values[1], values[0])

        def inside(row, key_row):
            return row - 4 <= key_row <= row + 3

        for row in range(ROWS):
            for m in range(0, ROWS, 2):
                penalties = tuple(
                    0.0 if inside(row, m + d) else (at_start if row < 4 else at_end)
                    for d in range(2)
                )
                own_bias[layer, row, :, m * GRID_W : (m + 2) * GRID_W] = pair(row, m, penalties)
            for m in range(0, 4, 2):
                lanes_at = slice(m * GRID_W, (m + 2) * GRID_W)
                if row < 4:
                    penalties = tuple(
                        not_start if inside(row, m + d - 4) else None for d in range(2)
                    )
                    low_bias[layer, row, :, lanes_at] = pair(row, m - 4, penalties)
                else:
                    penalties = tuple(not_end if inside(row, m + d + 8) else None for d in range(2))
                    high_bias[layer, row - 4, :, lanes_at] = pair(row, m + 8, penalties)

    pl.semaphore_wait(barrier, len(peers))

    def remote(src, dst, send_sem, recv_sem, device):
        return pltpu.make_async_remote_copy(
            src_ref=src,
            dst_ref=dst,
            send_sem=send_sem,
            recv_sem=recv_sem,
            device_id=device,
            device_id_type=MESH_ID,
        )

    def chunk_rows(chunk):
        start = chunk * PART
        return pl.ds(start if isinstance(chunk, int) else pl.multiple_of(start, PART), PART)

    def z_copy(layer, origin, part, step):
        c, chunk = part
        ref = xg.at[layer, origin, c, chunk_rows(chunk)]
        return remote(ref, ref, z_send.at[layer], z_recv.at[layer, step, c, chunk], z_onward)

    def core_copy(layer, origin, part):
        c, chunk = part
        ref = xg.at[layer, origin, c, chunk_rows(chunk)]
        return remote(ref, ref, core_send.at[layer], core_recv.at[layer, origin], sibling)

    def own_core_copy(layer, part):
        c, chunk = part
        ref = xg.at[layer, z, c, chunk_rows(chunk)]
        return remote(ref, ref, core_send.at[layer], own_recv.at[layer, chunk], sibling)

    own_parts = [(core, chunk) for chunk in range(CHUNKS)]
    other_parts = [(1 - core, chunk) for chunk in range(CHUNKS)]

    def gain_ref(origin, step):
        return gains.at[origin, core] if step == steps else gains.at[origin]

    def gain_copy(origin, step):
        ref = gain_ref(origin, step + 1)
        return remote(ref, ref, gain_send, gain_recv.at[step], z_onward)

    def gain_core_copy(ref, origin):
        return remote(ref, ref, gain_core_send, gain_core_recv.at[origin], sibling)

    def weight_round(action, layer, name):
        for link, (axis, sign) in enumerate(LINKS):
            device = {"sp": around(axis, sign, 0), "tp": tp}
            messages = [m for m in weight_messages(axis, sign) if m[0] == name]
            if action == "send":
                for _, sem, (along, across), piece, pieces in messages:
                    ref = weights.at[layer, around(axis, along, across), pl.ds(piece, pieces)]
                    recv = w_recv.at[layer, link, sem]
                    remote(ref, ref, w_send.at[layer], recv, device).start()
            else:
                for sem in sorted({m[1] for m in messages}):
                    pieces = sum(m[4] for m in messages if m[1] == sem)
                    ref = weights.at[layer, 0, pl.ds(0, pieces)]
                    recv = w_recv.at[layer, link, sem]
                    remote(ref, ref, w_send.at[layer], recv, device).wait_recv()

    def weight_rounds(layer, step, part):
        for action, which, name in WEIGHTS_AT.get((layer, step, part), ()):
            if (action, which, name) == ("send", 0, "0a"):
                for load in loads[5:]:
                    load.wait()
            weight_round(action, which, name)

    def await_sibling(layer, distance):
        origin = at_z(-way * distance)
        block = xg.at[layer, origin]
        if distance == steps:
            block = block.at[1 - core]
        remote(block, block, core_send.at[layer], core_recv.at[layer, origin], sibling).wait_recv()
        if layer == 0:
            ref = gains.at[origin, 1 - core] if distance == steps else gains.at[origin]
            gain_core_copy(ref, origin).wait_recv()

    def add_blocks(layer, offsets):
        distance = abs(offsets[0])
        if distance:
            await_sibling(layer, distance)
        origins = [at_z(offset) for offset in offsets]
        right, factors = [], []
        for origin in origins:
            columns = []
            for m in range(3):
                pieces = weights[layer, pl.ds(origin * shards, shards), :, m]
                columns.append(pieces.reshape(BLOCK, HEAD))
            right.append(jnp.concatenate(columns, axis=1))
            for c in range(2):
                factors.append(gains[origin, c].astype(jnp.float32)[layer : layer + 1])
        right = jnp.concatenate(right, axis=0)
        for top in range(0, TOK, 256):
            rows = slice(top, top + 256)
            squares, scaled = square[rows, :], []
            for i, origin in enumerate(origins):
                for c in range(2):
                    wide = xg[layer, origin, c, rows, :].astype(jnp.float32)
                    squares = squares + wide * wide
                    scaled.append((wide * factors[2 * i + c]).astype(jnp.bfloat16))
            square[rows, :] = squares
            acc[rows, :] += jnp.dot(
                jnp.concatenate(scaled, axis=1), right, preferred_element_type=jnp.float32
            )

    def own_gain_rows():
        loads[1].wait()
        loads[2].wait()
        spare = jnp.zeros((PAD - 2, HEAD), jnp.float32)
        both_gains = [own_gains[layer].astype(jnp.float32) for layer in range(2)]
        gains[z, core] = jnp.concatenate(both_gains + [spare]).astype(jnp.bfloat16)

    def gather_step(layer, step):
        origin = at_z(way * step)
        if step == 0 and layer == 0:
            for part in own_parts:
                z_copy(layer, z, part, 0).start()
                own_core_copy(layer, part).start()
        if layer == 0:
            if step == 0:
                own_gain_rows()
                gain_core_copy(gains.at[z, core], z).start()
                gain_core_copy(gains.at[z, 1 - core], z).wait_recv()
            else:
                gain_copy(origin, step - 1).wait_recv()
                gain_core_copy(gain_ref(origin, step), origin).start()
            if step < steps:
                gain_copy(origin, step).start()
        for index, part in enumerate(own_parts + other_parts):
            if step == 0:
                if index >= CHUNKS:
                    own_core_copy(layer, part).wait_recv()
                    z_copy(layer, z, part, 0).start()
            elif step < steps or index < CHUNKS:
                z_copy(layer, origin, part, step - 1).wait_recv()
                if step < steps - 1 or (step == steps - 1 and index < CHUNKS):
                    z_copy(layer, origin, part, step).start()
                core_copy(layer, origin, part).start()
            weight_rounds(layer, step, index)
            if (layer, step, index) in BLOCKS_AT:
                add_blocks(layer, BLOCKS_AT[layer, step, index])

    def project(layer):
        mean = jnp.sum(square[...], axis=1, keepdims=True) * (1.0 / features)
        scale = lax.rsqrt(mean + EPS)
        up, down = halo_copies(layer)
        for kind in range(2):
            part = acc[:, (1 + kind) * HEAD : (2 + kind) * HEAD]
            kv[layer, kind, LOW : LOW + TOK, :] = (part * scale).astype(jnp.bfloat16)
            if kind == 0:
                up[0].start()
                down[0].start()
        query[...] = (acc[:, :HEAD] * scale).astype(jnp.bfloat16)

    def halo_copies(layer):
        up, down = [], []
        for kind in range(2):
            both = kv.at[layer, kind]
            up.append(
                remote(
                    both.at[pl.ds(TOK, LOW)],
                    both.at[pl.ds(0, LOW)],
                    halo_send.at[layer, 0, kind],
                    halo_recv.at[layer, 0, kind],
                    sp_next,
                )
            )
            down.append(
                remote(
                    both.at[pl.ds(LOW, HIGH)],
                    both.at[pl.ds(LOW + TOK, HIGH)],
                    halo_send.at[layer, 1, kind],
                    halo_recv.at[layer, 1, kind],
                    sp_prev,
                )
            )
        return up, down

    def scores(layer, half, keys, bands):
        score = lax.dot_general(
            query[pl.ds(half * TOK // 2, TOK // 2), :],
            kv[layer, 0, keys, :],
            (((1,), (1,)), ((), ())),
            preferred_element_type=jnp.float32,
        )
        return score * (HEAD**-0.5) + jnp.concatenate(bands, axis=0)

    def mix(layer, weight, keys):
        return jnp.dot(
            weight.astype(jnp.bfloat16), kv[layer, 1, keys, :], preferred_element_type=jnp.float32
        )

    def attend_own(layer, half):
        keys = pl.ds(LOW, TOK)
        score = scores(layer, half, keys, [own_bias[layer, 4 * half + i] for i in range(4)])
        most = jnp.max(score, axis=1, keepdims=True)
        weight = jnp.exp(score - most)
        return most, jnp.sum(weight, axis=1, keepdims=True), mix(layer, weight, keys)

    def halo_keys(half):
        return pl.ds(0 if half == 0 else LOW + TOK, LOW)

    def halo_weights(layer, half, most):
        bias = low_bias if half == 0 else high_bias
        score = scores(layer, half, halo_keys(half), [bias[layer, i] for i in range(4)])
        over = jnp.maximum(most, jnp.max(score, axis=1, keepdims=True))
        return jnp.exp(score - over), jnp.exp(most - over)

    loads[0].wait()
    for layer in range(2):
        if layer == 1:
            acc[...] = jnp.zeros_like(acc)
            square[...] = jnp.zeros_like(square)
        for step in range(steps + 1):
            gather_step(layer, step)
            if layer == 0 and step == 0:
                for at in range(2):
                    loads[3 + at].wait()
                    build_bias(at)
                acc[...] = jnp.zeros_like(acc)
                square[...] = jnp.zeros_like(square)
        add_blocks(layer, (steps,))
        project(layer)
        halos = halo_copies(layer)
        own = [attend_own(layer, 0)]
        for halo in halos:
            halo[1].start()
        weight_rounds(layer, "halo", 0)
        own.append(attend_own(layer, 1))
        for halo in halos:
            halo[0].wait_recv()
        added = [halo_weights(layer, half, own[half][0]) for half in range(2)]
        for halo in halos:
            halo[1].wait_recv()
        for half in range(2):
            _, total, mixed = own[half]
            weight, kept = added[half]
            total = total * kept + jnp.sum(weight, axis=1, keepdims=True)
            attended = (mixed * kept + mix(layer, weight, halo_keys(half))) / total
            rows = pl.ds(half * TOK // 2, TOK // 2)
            x = xg[layer, z, core, rows, :].astype(jnp.float32)
            result = (x + attended).astype(jnp.bfloat16)
            if layer == 0:
                xg[1, z, core, rows, :] = result
                for part in own_parts[half * CHUNKS // 2 : (half + 1) * CHUNKS // 2]:
                    z_copy(1, z, part, 0).start()
                    own_core_copy(1, part).start()
            else:
                out[rows, :] = result

    sent = gains.at[pl.ds(0, zn - 1), 0]
    remote(sent, sent, gain_send, gain_recv.at[0], z_onward).wait_send()
    sent = gains.at[pl.ds(0, zn), 0]
    remote(sent, sent, gain_core_send, gain_core_recv.at[0], sibling).wait_send()
    for layer in range(2):
        sent = xg.at[layer, pl.ds(0, zn - 1), 0]
        remote(sent, sent, z_send.at[layer], z_recv.at[layer, 0, 0, 0], z_onward).wait_send()
        sent = xg.at[layer, pl.ds(0, zn), 0]
        remote(sent, sent, core_send.at[layer], core_recv.at[layer, 0], sibling).wait_send()
        sent = weights.at[layer, pl.ds(0, n_sp - 1)]
        remote(sent, sent, w_send.at[layer], w_recv.at[layer, 0, 0], sp_next).wait_send()
        for pair in halo_copies(layer):
            for copy in pair:
                copy.wait_send()


def body(zn, x, gain0, q0, k0, v0, table0, gain1, q1, k1, v1, table1):
    piece = q0.shape[0] // 4
    pieces = [w.reshape(4, piece, HEAD) for w in (q0, k0, v0, q1, k1, v1)]
    steps = zn // 2
    n_sp = SIDE * SIDE
    hbm = pl.BlockSpec(memory_space=pltpu.HBM)
    vmem = pl.BlockSpec(memory_space=pltpu.VMEM)
    dma = pltpu.SemaphoreType.DMA
    return pl.pallas_call(
        functools.partial(kernel, zn),
        out_shape=jax.ShapeDtypeStruct((TOK, HEAD), jnp.bfloat16),
        in_specs=[hbm] * 11,
        out_specs=vmem,
        scratch_shapes=[
            pltpu.VMEM((2, zn, 2, TOK, HEAD), jnp.bfloat16),
            pltpu.VMEM((2, n_sp, 4, 3, piece, HEAD), jnp.bfloat16),
            pltpu.VMEM((2, 2, LOW + TOK + 4 * GRID_W, HEAD), jnp.bfloat16),
            pltpu.VMEM((TOK, HEAD), jnp.bfloat16),
            pltpu.VMEM((TOK, 3 * HEAD), jnp.float32),
            pltpu.VMEM((TOK, HEAD), jnp.float32),
            pltpu.VMEM((2, 1, HEAD), jnp.bfloat16),
            pltpu.VMEM((zn, 2, PAD, HEAD), jnp.bfloat16),
            pltpu.VMEM((2, 15, 1, 31), jnp.float32),
            pltpu.VMEM((16, HEAD), jnp.float32),
            pltpu.VMEM((14, GRID_W, HEAD), jnp.float32),
            pltpu.VMEM((2, ROWS, GRID_W, TOK), jnp.float32),
            pltpu.VMEM((2, 4, GRID_W, LOW), jnp.float32),
            pltpu.VMEM((2, 4, GRID_W, LOW), jnp.float32),
            dma((11,)),
            dma((2,)),
            dma((2, steps, 2, CHUNKS)),
            dma((2,)),
            dma((2, zn)),
            dma((2, CHUNKS)),
            dma,
            dma((steps,)),
            dma,
            dma((zn,)),
            dma((2,)),
            dma((2, 4, 8)),
            dma((2, 2, 2)),
            dma((2, 2, 2)),
        ],
        compiler_params=pltpu.CompilerParams(
            collective_id=0, has_side_effects=True, vmem_limit_bytes=67043328
        ),
        name="neighbourhood",
    )(
        x,
        gain0.reshape(1, HEAD),
        gain1.reshape(1, HEAD),
        *pieces,
        jnp.swapaxes(table0, 0, 1),
        jnp.swapaxes(table1, 0, 1),
    )


def solution(mesh):
    placed = (
        P("sp", "tp"),
        P("tp"),
        P("sp", "tp"),
        P("sp", "tp"),
        P("sp", "tp"),
        P("tp", None, None),
        P("tp"),
        P("sp", "tp"),
        P("sp", "tp"),
        P("sp", "tp"),
        P("tp", None, None),
    )
    return jax.shard_map(
        functools.partial(body, mesh.shape["tp"] // 2),
        mesh=mesh,
        in_specs=placed,
        out_specs=P("sp", "tp"),
        check_vma=False,
    )
```

```python
import functools

import jax
import jax.numpy as jnp
from jax import lax
from jax.experimental import pallas as pl
from jax.experimental.pallas import tpu as pltpu
from jax.sharding import PartitionSpec as P

GRID_W = 64
HEAD = 128
ROWS = 8
TOK = ROWS * GRID_W
CHUNKS = 4
PART = TOK // CHUNKS
PAD = 16
SIDE = 4
EPS = 1e-6
BLOCK = 2 * HEAD
LOW = 4 * GRID_W
HIGH = 3 * GRID_W
X, Y = 0, 1
LINKS = ((X, 1), (X, -1), (Y, 1), (Y, -1))
MESH_ID = pl.DeviceIdType.MESH


def weight_messages(axis, sign):
    part = 0 if sign > 0 else 1
    half = 1 if axis == X else 0
    own_first = 0 if axis == X else 2
    return (
        ("0a", 0, (0, 0), own_first, 2),
        ("0b", 1, (0, 0), 2 - own_first, 2),
        ("1h", 2, (0, -1), 2 * half, 2),
        ("1h", 2, (0, 1), 2 * half, 2),
        ("1s", 3, (-sign, 0), own_first + part, 1),
        ("1b", 5, (-sign, 0), 2 - own_first + part, 1),
        ("2a", 4, (0, 2), 2 * half, 2),
        ("2b", 5, (-sign, -1), 2 * half + part, 1),
        ("2b", 5, (-sign, 1), 2 * half + part, 1),
        ("3", 5, (-sign, 2), 2 * half + part, 1),
    )


WEIGHTS_AT = {
    (0, 0, 7): (("send", 0, "0a"), ("send", 0, "0b")),
    (0, 1, 3): (("wait", 0, "0a"), ("send", 0, "1s")),
    (0, 1, 5): (("send", 0, "1h"),),
    (0, 3, 0): (("wait", 0, "1s"), ("send", 0, "2a")),
    (0, 4, 3): (("wait", 0, "1h"), ("send", 0, "2b"), ("wait", 0, "0b"), ("send", 0, "1b")),
    (0, 5, 1): (("wait", 0, "2a"), ("send", 0, "3")),
    (0, 6, 5): (("wait", 0, "3"), ("send", 1, "0a"), ("send", 1, "0b")),
    (0, 8, 3): (("wait", 1, "0a"), ("send", 1, "1s")),
    (0, "halo", 0): (
        ("wait", 1, "1s"),
        ("send", 1, "2a"),
        ("send", 1, "1h"),
        ("wait", 1, "0b"),
        ("send", 1, "1b"),
    ),
    (1, 1, 5): (("wait", 1, "2a"), ("send", 1, "3")),
    (1, 3, 1): (("wait", 1, "1h"), ("send", 1, "2b")),
    (1, 5, 0): (("wait", 1, "3"),),
}
BLOCKS_AT = {
    (0, 6, 6): (0,),
    (0, 6, 7): (-1, 1),
    (0, 7, 0): (-2, 2),
    (0, 7, 1): (-3, 3),
    (0, 7, 3): (-4, 4),
    (0, 7, 5): (-5, 5),
    (0, 7, 7): (-6, 6),
    (0, 8, 2): (-7, 7),
    (1, 5, 1): (0,),
    (1, 5, 2): (-1, 1),
    (1, 5, 4): (-2, 2),
    (1, 5, 6): (-3, 3),
    (1, 6, 2): (-4, 4),
    (1, 6, 6): (-5, 5),
    (1, 7, 5): (-6, 6),
    (1, 8, 3): (-7, 7),
}
MASKED = -1e30


def kernel(
    zn,
    x_hbm,
    gain0_hbm,
    gain1_hbm,
    q0_hbm,
    k0_hbm,
    v0_hbm,
    q1_hbm,
    k1_hbm,
    v1_hbm,
    table0_hbm,
    table1_hbm,
    out,
    xg,
    weights,
    kv,
    query,
    acc,
    square,
    own_gains,
    gains,
    tables,
    tab,
    band,
    own_bias,
    low_bias,
    high_bias,
    result_buffer,
    local_sem,
    z_send,
    z_recv,
    core_send,
    core_recv,
    own_recv,
    gain_send,
    gain_recv,
    gain_core_send,
    gain_core_recv,
    w_send,
    w_recv,
    halo_send,
    halo_recv,
):
    sp = lax.axis_index("sp")
    tp = lax.axis_index("tp")
    n_sp = SIDE * SIDE
    gx, gy = lax.rem(sp, SIDE), lax.div(sp, SIDE)
    core, z = lax.rem(tp, 2), lax.div(tp, 2)
    steps = zn // 2
    shards = n_sp // zn
    features = zn * BLOCK

    def at_z(offset):
        return lax.rem(z + offset + zn, zn)

    def chip(z_at, core_at):
        return {"sp": sp, "tp": z_at * 2 + core_at}

    def grid_sp(dx, dy):
        return lax.rem(gy + dy + SIDE, SIDE) * SIDE + lax.rem(gx + dx + SIDE, SIDE)

    def around(axis, along, across):
        along, across = (along + SIDE) % SIDE, (across + SIDE) % SIDE
        return grid_sp(along, across) if axis == X else grid_sp(across, along)

    sibling = chip(z, 1 - core)
    way = 2 * core - 1
    z_onward, z_source = chip(at_z(-way), core), chip(at_z(way), core)
    sp_next = {"sp": lax.rem(sp + 1, n_sp), "tp": tp}
    sp_prev = {"sp": lax.rem(sp + n_sp - 1, n_sp), "tp": tp}

    barrier = pltpu.get_barrier_semaphore()
    peers = [z_source, sibling, sp_next, sp_prev]
    peers += [{"sp": around(axis, sign, 0), "tp": tp} for axis, sign in LINKS]
    for peer in peers:
        pl.semaphore_signal(barrier, inc=1, device_id=peer, device_id_type=MESH_ID)

    loads = [
        pltpu.make_async_copy(x_hbm, xg.at[0, z, core], local_sem.at[0]),
        pltpu.make_async_copy(gain0_hbm, own_gains.at[0], local_sem.at[1]),
        pltpu.make_async_copy(gain1_hbm, own_gains.at[1], local_sem.at[2]),
        pltpu.make_async_copy(table0_hbm, tables.at[0], local_sem.at[3]),
        pltpu.make_async_copy(table1_hbm, tables.at[1], local_sem.at[4]),
    ]
    for layer, refs in enumerate(((q0_hbm, k0_hbm, v0_hbm), (q1_hbm, k1_hbm, v1_hbm))):
        for m, ref in enumerate(refs):
            loads.append(
                pltpu.make_async_copy(
                    ref, weights.at[layer, sp, :, m], local_sem.at[5 + 3 * layer + m]
                )
            )
    for load in loads:
        load.start()

    for layer in range(2):
        kv[layer, :, LOW + TOK + HIGH :, :] = jnp.zeros((2, GRID_W, HEAD), jnp.bfloat16)

    def build_bias(layer):
        lanes = lax.broadcasted_iota(jnp.int32, (GRID_W, HEAD), 1)
        key_column = lanes & (GRID_W - 1)
        column = lax.broadcasted_iota(jnp.int32, (GRID_W, HEAD), 0)
        first_column = jnp.clip(column - 8, 0, GRID_W - 16)
        in_window = (key_column >= first_column) & (key_column < first_column + 16)
        tab[...] = jnp.zeros_like(tab)
        tab[0:15, 0:31] = tables[layer, :, 0, :]
        rows = tab[...]
        both = rows + pltpu.roll(pltpu.roll(rows, 15, 0), GRID_W, 1)
        for offset in range(14):
            spread = jnp.broadcast_to(both[offset : offset + 1], (GRID_W, HEAD))
            shifted = pltpu.roll(spread, HEAD - 15, 1, stride=1, stride_axis=0)
            band[offset] = jnp.where(in_window, shifted, MASKED)
        at_start = jnp.where(sp == 0, 0.0, MASKED)
        at_end = jnp.where(sp == n_sp - 1, 0.0, MASKED)
        not_start = jnp.where(sp == 0, MASKED, 0.0)
        not_end = jnp.where(sp == n_sp - 1, MASKED, 0.0)
        right = lanes >= GRID_W

        def pair(row, key_row, penalties):
            if penalties == (None, None):
                return jnp.full((GRID_W, HEAD), MASKED, jnp.float32)
            values = [MASKED if p is None else p for p in penalties]
            offset = key_row - row + 7
            base = band[offset]
            return base + jnp.where(right, values[1], values[0])

        def inside(row, key_row):
            return row - 4 <= key_row <= row + 3

        for row in range(ROWS):
            for m in range(0, ROWS, 2):
                penalties = tuple(
                    0.0 if inside(row, m + d) else (at_start if row < 4 else at_end)
                    for d in range(2)
                )
                own_bias[layer, row, :, m * GRID_W : (m + 2) * GRID_W] = pair(row, m, penalties)
            for m in range(0, 4, 2):
                lanes_at = slice(m * GRID_W, (m + 2) * GRID_W)
                if row < 4:
                    penalties = tuple(
                        not_start if inside(row, m + d - 4) else None for d in range(2)
                    )
                    low_bias[layer, row, :, lanes_at] = pair(row, m - 4, penalties)
                else:
                    penalties = tuple(not_end if inside(row, m + d + 8) else None for d in range(2))
                    high_bias[layer, row - 4, :, lanes_at] = pair(row, m + 8, penalties)

    pl.semaphore_wait(barrier, len(peers))

    def remote(src, dst, send_sem, recv_sem, device):
        return pltpu.make_async_remote_copy(
            src_ref=src,
            dst_ref=dst,
            send_sem=send_sem,
            recv_sem=recv_sem,
            device_id=device,
            device_id_type=MESH_ID,
        )

    def chunk_rows(chunk):
        start = chunk * PART
        return pl.ds(start if isinstance(chunk, int) else pl.multiple_of(start, PART), PART)

    def z_copy(layer, origin, part, step):
        c, chunk = part
        ref = xg.at[layer, origin, c, chunk_rows(chunk)]
        return remote(ref, ref, z_send.at[layer], z_recv.at[layer, step, c, chunk], z_onward)

    def core_copy(layer, origin, part):
        c, chunk = part
        ref = xg.at[layer, origin, c, chunk_rows(chunk)]
        return remote(ref, ref, core_send.at[layer], core_recv.at[layer, origin], sibling)

    def own_core_copy(layer, part):
        c, chunk = part
        ref = xg.at[layer, z, c, chunk_rows(chunk)]
        return remote(ref, ref, core_send.at[layer], own_recv.at[layer, chunk], sibling)

    own_parts = [(core, chunk) for chunk in range(CHUNKS)]
    other_parts = [(1 - core, chunk) for chunk in range(CHUNKS)]

    def gain_ref(origin, step):
        return gains.at[origin, core] if step == steps else gains.at[origin]

    def gain_copy(origin, step):
        ref = gain_ref(origin, step + 1)
        return remote(ref, ref, gain_send, gain_recv.at[step], z_onward)

    def gain_core_copy(ref, origin):
        return remote(ref, ref, gain_core_send, gain_core_recv.at[origin], sibling)

    def weight_round(action, layer, name):
        for link, (axis, sign) in enumerate(LINKS):
            device = {"sp": around(axis, sign, 0), "tp": tp}
            messages = weight_messages(axis, sign)
            if action == "send":
                messages = [m for m in messages if m[0] == name]
                for _, sem, (along, across), piece, pieces in messages:
                    ref = weights.at[layer, around(axis, along, across), pl.ds(piece, pieces)]
                    recv = w_recv.at[layer, link, sem]
                    remote(ref, ref, w_send.at[layer], recv, device).start()
            else:
                (sem,) = {m[1] for m in messages if m[0] == name}
                pieces = sum(m[4] for m in messages if m[1] == sem)
                ref = weights.at[layer, 0, pl.ds(0, pieces)]
                recv = w_recv.at[layer, link, sem]
                remote(ref, ref, w_send.at[layer], recv, device).wait_recv()

    def weight_rounds(layer, step, part):
        for action, which, name in WEIGHTS_AT.get((layer, step, part), ()):
            if (action, which, name) == ("send", 0, "0a"):
                for load in loads[5:]:
                    load.wait()
            weight_round(action, which, name)

    def await_sibling(layer, distance):
        origin = at_z(-way * distance)
        block = xg.at[layer, origin]
        if distance == steps:
            block = block.at[1 - core]
        remote(block, block, core_send.at[layer], core_recv.at[layer, origin], sibling).wait_recv()
        if layer == 0:
            ref = gains.at[origin, 1 - core] if distance == steps else gains.at[origin]
            gain_core_copy(ref, origin).wait_recv()

    def add_blocks(layer, offsets):
        distance = abs(offsets[0])
        if distance:
            await_sibling(layer, distance)
        origins = [at_z(offset) for offset in offsets]
        right, factors = [], []
        for origin in origins:
            columns = []
            for m in range(3):
                pieces = weights[layer, pl.ds(origin * shards, shards), :, m]
                columns.append(pieces.reshape(BLOCK, HEAD))
            right.append(jnp.concatenate(columns, axis=1))
            for c in range(2):
                factors.append(gains[origin, c].astype(jnp.float32)[layer : layer + 1])
        right = jnp.concatenate(right, axis=0)
        for top in range(0, TOK, 256):
            rows = slice(top, top + 256)
            squares, scaled = square[rows, :], []
            for i, origin in enumerate(origins):
                for c in range(2):
                    wide = xg[layer, origin, c, rows, :].astype(jnp.float32)
                    squares = squares + wide * wide
                    scaled.append((wide * factors[2 * i + c]).astype(jnp.bfloat16))
            square[rows, :] = squares
            acc[rows, :] += jnp.dot(
                jnp.concatenate(scaled, axis=1), right, preferred_element_type=jnp.float32
            )

    def own_gain_rows():
        loads[1].wait()
        loads[2].wait()
        spare = jnp.zeros((PAD - 2, HEAD), jnp.float32)
        both_gains = [own_gains[layer].astype(jnp.float32) for layer in range(2)]
        gains[z, core] = jnp.concatenate(both_gains + [spare]).astype(jnp.bfloat16)

    def gather_step(layer, step):
        origin = at_z(way * step)
        if step == 0 and layer == 0:
            for part in own_parts:
                z_copy(layer, z, part, 0).start()
                own_core_copy(layer, part).start()
        if layer == 0:
            if step == 0:
                own_gain_rows()
                gain_core_copy(gains.at[z, core], z).start()
                gain_core_copy(gains.at[z, 1 - core], z).wait_recv()
            else:
                gain_copy(origin, step - 1).wait_recv()
                gain_core_copy(gain_ref(origin, step), origin).start()
            if step < steps:
                gain_copy(origin, step).start()
        for index, part in enumerate(own_parts + other_parts):
            if step == 0:
                if index >= CHUNKS:
                    own_core_copy(layer, part).wait_recv()
                    z_copy(layer, z, part, 0).start()
            elif step < steps or index < CHUNKS:
                z_copy(layer, origin, part, step - 1).wait_recv()
                if step < steps - 1 or (step == steps - 1 and index < CHUNKS):
                    z_copy(layer, origin, part, step).start()
                core_copy(layer, origin, part).start()
            weight_rounds(layer, step, index)
            if (layer, step, index) in BLOCKS_AT:
                add_blocks(layer, BLOCKS_AT[layer, step, index])

    def project(layer):
        mean = jnp.sum(square[...], axis=1, keepdims=True) * (1.0 / features)
        scale = lax.rsqrt(mean + EPS)
        for kind in range(2):
            part = acc[:, (1 + kind) * HEAD : (2 + kind) * HEAD]
            kv[layer, kind, LOW : LOW + TOK, :] = (part * scale).astype(jnp.bfloat16)
            if kind == 0:
                for halo in halo_copies(layer, 0):
                    halo.start()
        query[...] = (acc[:, :HEAD] * scale).astype(jnp.bfloat16)

    def halo_copies(layer, kind):
        both = kv.at[layer, kind]
        up = remote(
            both.at[pl.ds(TOK, LOW)],
            both.at[pl.ds(0, LOW)],
            halo_send.at[layer, 0, kind],
            halo_recv.at[layer, 0, kind],
            sp_next,
        )
        down = remote(
            both.at[pl.ds(LOW, HIGH)],
            both.at[pl.ds(LOW + TOK, HIGH)],
            halo_send.at[layer, 1, kind],
            halo_recv.at[layer, 1, kind],
            sp_prev,
        )
        return up, down

    def scores(layer, half, keys, bands):
        score = lax.dot_general(
            query[pl.ds(half * TOK // 2, TOK // 2), :],
            kv[layer, 0, keys, :],
            (((1,), (1,)), ((), ())),
            preferred_element_type=jnp.float32,
        )
        return score * (HEAD**-0.5) + jnp.concatenate(bands, axis=0)

    def mix(layer, weight, keys):
        return jnp.dot(
            weight.astype(jnp.bfloat16), kv[layer, 1, keys, :], preferred_element_type=jnp.float32
        )

    def attend_own(layer, half):
        keys = pl.ds(LOW, TOK)
        score = scores(layer, half, keys, [own_bias[layer, 4 * half + i] for i in range(4)])
        most = jnp.max(score, axis=1, keepdims=True)
        weight = jnp.exp(score - most)
        return most, jnp.sum(weight, axis=1, keepdims=True), mix(layer, weight, keys)

    def halo_keys(half):
        return pl.ds(0 if half == 0 else LOW + TOK, LOW)

    def halo_weights(layer, half, most):
        bias = low_bias if half == 0 else high_bias
        score = scores(layer, half, halo_keys(half), [bias[layer, i] for i in range(4)])
        over = jnp.maximum(most, jnp.max(score, axis=1, keepdims=True))
        return jnp.exp(score - over), jnp.exp(most - over)

    outs = [
        pltpu.make_async_copy(
            result_buffer.at[pl.ds(half * TOK // 2, TOK // 2)],
            out.at[pl.ds(half * TOK // 2, TOK // 2)],
            local_sem.at[11 + half],
        )
        for half in range(2)
    ]

    loads[0].wait()
    for layer in range(2):
        if layer == 1:
            acc[...] = jnp.zeros_like(acc)
            square[...] = jnp.zeros_like(square)
        for step in range(steps + 1):
            gather_step(layer, step)
            if layer == 0 and step == 0:
                for at in range(2):
                    loads[3 + at].wait()
                    build_bias(at)
                acc[...] = jnp.zeros_like(acc)
                square[...] = jnp.zeros_like(square)
        add_blocks(layer, (steps,))
        project(layer)
        own = [attend_own(layer, 0)]
        for halo in halo_copies(layer, 1):
            halo.start()
        own.append(attend_own(layer, 1))
        for halo in halo_copies(layer, 0):
            halo.wait_recv()
        weight_rounds(layer, "halo", 0)
        added = [halo_weights(layer, half, own[half][0]) for half in range(2)]
        for halo in halo_copies(layer, 1):
            halo.wait_recv()
        for half in range(2):
            _, total, mixed = own[half]
            weight, kept = added[half]
            total = total * kept + jnp.sum(weight, axis=1, keepdims=True)
            attended = (mixed * kept + mix(layer, weight, halo_keys(half))) / total
            rows = pl.ds(half * TOK // 2, TOK // 2)
            x = xg[layer, z, core, rows, :].astype(jnp.float32)
            result = (x + attended).astype(jnp.bfloat16)
            if layer == 0:
                xg[1, z, core, rows, :] = result
                for part in own_parts[half * CHUNKS // 2 : (half + 1) * CHUNKS // 2]:
                    z_copy(1, z, part, 0).start()
                    own_core_copy(1, part).start()
            else:
                result_buffer[rows, :] = result
                outs[half].start()

    for copy in outs:
        copy.wait()
    sent = gains.at[pl.ds(0, zn - 1), 0]
    remote(sent, sent, gain_send, gain_recv.at[0], z_onward).wait_send()
    sent = gains.at[pl.ds(0, zn), 0]
    remote(sent, sent, gain_core_send, gain_core_recv.at[0], sibling).wait_send()
    for layer in range(2):
        sent = xg.at[layer, pl.ds(0, zn - 1), 0]
        remote(sent, sent, z_send.at[layer], z_recv.at[layer, 0, 0, 0], z_onward).wait_send()
        sent = xg.at[layer, pl.ds(0, zn), 0]
        remote(sent, sent, core_send.at[layer], core_recv.at[layer, 0], sibling).wait_send()
        sent = weights.at[layer, pl.ds(0, n_sp - 1)]
        remote(sent, sent, w_send.at[layer], w_recv.at[layer, 0, 0], sp_next).wait_send()
        for kind in range(2):
            for halo in halo_copies(layer, kind):
                halo.wait_send()


def body(zn, x, gain0, q0, k0, v0, table0, gain1, q1, k1, v1, table1):
    piece = q0.shape[0] // 4
    pieces = [w.reshape(4, piece, HEAD) for w in (q0, k0, v0, q1, k1, v1)]
    steps = zn // 2
    n_sp = SIDE * SIDE
    hbm = pl.BlockSpec(memory_space=pltpu.HBM)
    dma = pltpu.SemaphoreType.DMA
    return pl.pallas_call(
        functools.partial(kernel, zn),
        out_shape=jax.ShapeDtypeStruct((TOK, HEAD), jnp.bfloat16),
        in_specs=[hbm] * 11,
        out_specs=hbm,
        scratch_shapes=[
            pltpu.VMEM((2, zn, 2, TOK, HEAD), jnp.bfloat16),
            pltpu.VMEM((2, n_sp, 4, 3, piece, HEAD), jnp.bfloat16),
            pltpu.VMEM((2, 2, LOW + TOK + 4 * GRID_W, HEAD), jnp.bfloat16),
            pltpu.VMEM((TOK, HEAD), jnp.bfloat16),
            pltpu.VMEM((TOK, 3 * HEAD), jnp.float32),
            pltpu.VMEM((TOK, HEAD), jnp.float32),
            pltpu.VMEM((2, 1, HEAD), jnp.bfloat16),
            pltpu.VMEM((zn, 2, PAD, HEAD), jnp.bfloat16),
            pltpu.VMEM((2, 15, 1, 31), jnp.float32),
            pltpu.VMEM((16, HEAD), jnp.float32),
            pltpu.VMEM((14, GRID_W, HEAD), jnp.float32),
            pltpu.VMEM((2, ROWS, GRID_W, TOK), jnp.float32),
            pltpu.VMEM((2, 4, GRID_W, LOW), jnp.float32),
            pltpu.VMEM((2, 4, GRID_W, LOW), jnp.float32),
            pltpu.VMEM((TOK, HEAD), jnp.bfloat16),
            dma((13,)),
            dma((2,)),
            dma((2, steps, 2, CHUNKS)),
            dma((2,)),
            dma((2, zn)),
            dma((2, CHUNKS)),
            dma,
            dma((steps,)),
            dma,
            dma((zn,)),
            dma((2,)),
            dma((2, 4, 6)),
            dma((2, 2, 2)),
            dma((2, 2, 2)),
        ],
        compiler_params=pltpu.CompilerParams(
            collective_id=0, has_side_effects=True, vmem_limit_bytes=67043328
        ),
        name="neighbourhood",
    )(
        x,
        gain0.reshape(1, HEAD),
        gain1.reshape(1, HEAD),
        *pieces,
        jnp.swapaxes(table0, 0, 1),
        jnp.swapaxes(table1, 0, 1),
    )


def solution(mesh):
    placed = (
        P("sp", "tp"),
        P("tp"),
        P("sp", "tp"),
        P("sp", "tp"),
        P("sp", "tp"),
        P("tp", None, None),
        P("tp"),
        P("sp", "tp"),
        P("sp", "tp"),
        P("sp", "tp"),
        P("tp", None, None),
    )
    return jax.shard_map(
        functools.partial(body, mesh.shape["tp"] // 2),
        mesh=mesh,
        in_specs=placed,
        out_specs=P("sp", "tp"),
        check_vma=False,
    )
```

```python
import functools

import jax
import jax.numpy as jnp
from jax import lax
from jax.experimental import pallas as pl
from jax.experimental.pallas import tpu as pltpu
from jax.sharding import PartitionSpec as P

GRID_W = 64
HEAD = 128
ROWS = 8
TOK = ROWS * GRID_W
CHUNKS = 4
PART = TOK // CHUNKS
PAD = 16
SIDE = 4
EPS = 1e-6
BLOCK = 2 * HEAD
LOW = 4 * GRID_W
HIGH = 3 * GRID_W
X, Y = 0, 1
LINKS = ((X, 1), (X, -1), (Y, 1), (Y, -1))
MESH_ID = pl.DeviceIdType.MESH


def weight_messages(axis, sign):
    part = 0 if sign > 0 else 1
    half = 1 if axis == X else 0
    own_first = 0 if axis == X else 2
    return (
        ("0a", 0, (0, 0), own_first, 2),
        ("0b", 1, (0, 0), 2 - own_first, 2),
        ("1h", 2, (0, -1), 2 * half, 2),
        ("1h", 2, (0, 1), 2 * half, 2),
        ("1s", 3, (-sign, 0), own_first + part, 1),
        ("1b", 5, (-sign, 0), 2 - own_first + part, 1),
        ("2a", 4, (0, 2), 2 * half, 2),
        ("2b", 5, (-sign, -1), 2 * half + part, 1),
        ("2b", 5, (-sign, 1), 2 * half + part, 1),
        ("3", 5, (-sign, 2), 2 * half + part, 1),
    )


WEIGHTS_AT = {
    (0, 0, 7): (("send", 0, "0a"), ("send", 0, "0b")),
    (0, 1, 3): (("wait", 0, "0a"), ("send", 0, "1s")),
    (0, 1, 5): (("send", 0, "1h"),),
    (0, 3, 0): (("wait", 0, "1s"), ("send", 0, "2a")),
    (0, 4, 3): (("wait", 0, "1h"), ("send", 0, "2b"), ("wait", 0, "0b"), ("send", 0, "1b")),
    (0, 5, 1): (("wait", 0, "2a"), ("send", 0, "3")),
    (0, 6, 5): (("wait", 0, "3"), ("send", 1, "0a"), ("send", 1, "0b")),
    (0, 8, 3): (("wait", 1, "0a"), ("send", 1, "1s")),
    (0, "halo", 0): (
        ("wait", 1, "1s"),
        ("send", 1, "2a"),
        ("send", 1, "1h"),
        ("wait", 1, "0b"),
        ("send", 1, "1b"),
    ),
    (1, 1, 5): (("wait", 1, "2a"), ("send", 1, "3")),
    (1, 3, 1): (("wait", 1, "1h"), ("send", 1, "2b")),
    (1, 5, 0): (("wait", 1, "3"),),
}
BLOCKS_AT = {
    (0, 6, 6): (0,),
    (0, 7, 0): (-1, 1),
    (0, 7, 3): (-2, 2),
    (0, 7, 4): (-3, 3),
    (0, 7, 5): (-4, 4),
    (0, 7, 6): (-5, 5),
    (0, 7, 7): (-6, 6),
    (0, 8, 1): (-7, 7),
    (1, 5, 3): (0,),
    (1, 5, 6): (-1, 1),
    (1, 6, 1): (-2, 2),
    (1, 6, 5): (-3, 3),
    (1, 7, 3): (-4, 4),
    (1, 7, 4): (-5, 5),
    (1, 7, 6): (-6, 6),
    (1, 8, 1): (-7, 7),
}
MASKED = -1e30


def kernel(
    zn,
    x_hbm,
    gain0_hbm,
    gain1_hbm,
    q0_hbm,
    k0_hbm,
    v0_hbm,
    q1_hbm,
    k1_hbm,
    v1_hbm,
    table0_hbm,
    table1_hbm,
    out,
    xg,
    weights,
    kv,
    query,
    acc,
    square,
    own_gains,
    gains,
    tables,
    tab,
    band,
    own_bias,
    low_bias,
    high_bias,
    local_sem,
    z_send,
    z_recv,
    core_send,
    core_recv,
    own_recv,
    next_layer,
    gain_send,
    gain_recv,
    gain_core_send,
    gain_core_recv,
    w_send,
    w_recv,
    halo_send,
    halo_recv,
):
    sp = lax.axis_index("sp")
    tp = lax.axis_index("tp")
    n_sp = SIDE * SIDE
    gx, gy = lax.rem(sp, SIDE), lax.div(sp, SIDE)
    core, z = lax.rem(tp, 2), lax.div(tp, 2)
    steps = zn // 2
    shards = n_sp // zn
    features = zn * BLOCK

    def at_z(offset):
        return lax.rem(z + offset + zn, zn)

    def chip(z_at, core_at):
        return {"sp": sp, "tp": z_at * 2 + core_at}

    def grid_sp(dx, dy):
        return lax.rem(gy + dy + SIDE, SIDE) * SIDE + lax.rem(gx + dx + SIDE, SIDE)

    def around(axis, along, across):
        along, across = (along + SIDE) % SIDE, (across + SIDE) % SIDE
        return grid_sp(along, across) if axis == X else grid_sp(across, along)

    sibling = chip(z, 1 - core)
    way = 2 * core - 1
    z_onward, z_source = chip(at_z(-way), core), chip(at_z(way), core)
    sp_next = {"sp": lax.rem(sp + 1, n_sp), "tp": tp}
    sp_prev = {"sp": lax.rem(sp + n_sp - 1, n_sp), "tp": tp}

    barrier = pltpu.get_barrier_semaphore()
    peers = [z_source, sibling, sp_next, sp_prev]
    peers += [{"sp": around(axis, sign, 0), "tp": tp} for axis, sign in LINKS]
    for peer in peers:
        pl.semaphore_signal(barrier, inc=1, device_id=peer, device_id_type=MESH_ID)

    loads = [
        pltpu.make_async_copy(x_hbm, xg.at[0, z, core], local_sem.at[0]),
        pltpu.make_async_copy(gain0_hbm, own_gains.at[0], local_sem.at[1]),
        pltpu.make_async_copy(gain1_hbm, own_gains.at[1], local_sem.at[2]),
        pltpu.make_async_copy(table0_hbm, tables.at[0], local_sem.at[3]),
        pltpu.make_async_copy(table1_hbm, tables.at[1], local_sem.at[4]),
    ]
    for layer, refs in enumerate(((q0_hbm, k0_hbm, v0_hbm), (q1_hbm, k1_hbm, v1_hbm))):
        for m, ref in enumerate(refs):
            loads.append(
                pltpu.make_async_copy(
                    ref, weights.at[layer, sp, :, m], local_sem.at[5 + 3 * layer + m]
                )
            )
    for load in loads:
        load.start()

    for layer in range(2):
        kv[layer, :, LOW + TOK + HIGH :, :] = jnp.zeros((2, GRID_W, HEAD), jnp.bfloat16)

    def build_bias(layer):
        lanes = lax.broadcasted_iota(jnp.int32, (GRID_W, HEAD), 1)
        key_column = lanes & (GRID_W - 1)
        column = lax.broadcasted_iota(jnp.int32, (GRID_W, HEAD), 0)
        first_column = jnp.clip(column - 8, 0, GRID_W - 16)
        in_window = (key_column >= first_column) & (key_column < first_column + 16)
        tab[...] = jnp.zeros_like(tab)
        tab[0:15, 0:31] = tables[layer, :, 0, :]
        rows = tab[...]
        both = rows + pltpu.roll(pltpu.roll(rows, 15, 0), GRID_W, 1)
        for offset in range(14):
            spread = jnp.broadcast_to(both[offset : offset + 1], (GRID_W, HEAD))
            shifted = pltpu.roll(spread, HEAD - 15, 1, stride=1, stride_axis=0)
            band[offset] = jnp.where(in_window, shifted, MASKED)
        at_start = jnp.where(sp == 0, 0.0, MASKED)
        at_end = jnp.where(sp == n_sp - 1, 0.0, MASKED)
        not_start = jnp.where(sp == 0, MASKED, 0.0)
        not_end = jnp.where(sp == n_sp - 1, MASKED, 0.0)
        right = lanes >= GRID_W

        def pair(row, key_row, penalties):
            if penalties == (None, None):
                return jnp.full((GRID_W, HEAD), MASKED, jnp.float32)
            values = [MASKED if p is None else p for p in penalties]
            offset = key_row - row + 7
            base = band[offset]
            return base + jnp.where(right, values[1], values[0])

        def inside(row, key_row):
            return row - 4 <= key_row <= row + 3

        for row in range(ROWS):
            for m in range(0, ROWS, 2):
                penalties = tuple(
                    0.0 if inside(row, m + d) else (at_start if row < 4 else at_end)
                    for d in range(2)
                )
                own_bias[layer, row, :, m * GRID_W : (m + 2) * GRID_W] = pair(row, m, penalties)
            for m in range(0, 4, 2):
                lanes_at = slice(m * GRID_W, (m + 2) * GRID_W)
                if row < 4:
                    penalties = tuple(
                        not_start if inside(row, m + d - 4) else None for d in range(2)
                    )
                    low_bias[layer, row, :, lanes_at] = pair(row, m - 4, penalties)
                else:
                    penalties = tuple(not_end if inside(row, m + d + 8) else None for d in range(2))
                    high_bias[layer, row - 4, :, lanes_at] = pair(row, m + 8, penalties)

    pl.semaphore_wait(barrier, len(peers))

    def remote(src, dst, send_sem, recv_sem, device):
        return pltpu.make_async_remote_copy(
            src_ref=src,
            dst_ref=dst,
            send_sem=send_sem,
            recv_sem=recv_sem,
            device_id=device,
            device_id_type=MESH_ID,
        )

    def chunk_rows(chunk):
        start = chunk * PART
        return pl.ds(start if isinstance(chunk, int) else pl.multiple_of(start, PART), PART)

    def z_copy(layer, origin, part, step):
        c, chunk = part
        ref = xg.at[layer, origin, c, chunk_rows(chunk)]
        return remote(ref, ref, z_send.at[layer], z_recv.at[step, c, chunk], z_onward)

    def core_copy(layer, origin, part):
        c, chunk = part
        ref = xg.at[layer, origin, c, chunk_rows(chunk)]
        return remote(ref, ref, core_send.at[layer], core_recv.at[origin], sibling)

    def own_core_copy(layer, part):
        c, chunk = part
        ref = xg.at[layer, z, c, chunk_rows(chunk)]
        return remote(ref, ref, core_send.at[layer], own_recv.at[chunk], sibling)

    own_parts = [(core, chunk) for chunk in range(CHUNKS)]
    other_parts = [(1 - core, chunk) for chunk in range(CHUNKS)]

    def gain_ref(origin, step):
        return gains.at[origin, core] if step == steps else gains.at[origin]

    def gain_copy(origin, step):
        ref = gain_ref(origin, step + 1)
        return remote(ref, ref, gain_send, gain_recv.at[step], z_onward)

    def gain_core_copy(ref, origin):
        return remote(ref, ref, gain_core_send, gain_core_recv.at[origin], sibling)

    def weight_round(action, layer, name):
        for link, (axis, sign) in enumerate(LINKS):
            device = {"sp": around(axis, sign, 0), "tp": tp}
            messages = weight_messages(axis, sign)
            if action == "send":
                messages = [m for m in messages if m[0] == name]
                for _, sem, (along, across), piece, pieces in messages:
                    ref = weights.at[layer, around(axis, along, across), pl.ds(piece, pieces)]
                    recv = w_recv.at[layer, link, sem]
                    remote(ref, ref, w_send.at[layer], recv, device).start()
            else:
                (sem,) = {m[1] for m in messages if m[0] == name}
                pieces = sum(m[4] for m in messages if m[1] == sem)
                ref = weights.at[layer, 0, pl.ds(0, pieces)]
                recv = w_recv.at[layer, link, sem]
                remote(ref, ref, w_send.at[layer], recv, device).wait_recv()

    def weight_rounds(layer, step, part):
        for action, which, name in WEIGHTS_AT.get((layer, step, part), ()):
            if (action, which, name) == ("send", 0, "0a"):
                for load in loads[5:]:
                    load.wait()
            weight_round(action, which, name)

    def await_sibling(layer, distance):
        origin = at_z(-way * distance)
        block = xg.at[layer, origin]
        if distance == steps:
            block = block.at[1 - core]
        remote(block, block, core_send.at[layer], core_recv.at[origin], sibling).wait_recv()
        if layer == 0:
            ref = gains.at[origin, 1 - core] if distance == steps else gains.at[origin]
            gain_core_copy(ref, origin).wait_recv()

    def add_blocks(layer, offsets):
        distance = abs(offsets[0])
        if distance:
            await_sibling(layer, distance)
        origins = [at_z(offset) for offset in offsets]
        right, factors = [], []
        for origin in origins:
            columns = []
            for m in range(3):
                pieces = weights[layer, pl.ds(origin * shards, shards), :, m]
                columns.append(pieces.reshape(BLOCK, HEAD))
            right.append(jnp.concatenate(columns, axis=1))
            for c in range(2):
                factors.append(gains[origin, c].astype(jnp.float32)[layer : layer + 1])
        right = jnp.concatenate(right, axis=0)
        for top in range(0, TOK, 256):
            rows = slice(top, top + 256)
            squares, scaled = square[rows, :], []
            for i, origin in enumerate(origins):
                for c in range(2):
                    wide = xg[layer, origin, c, rows, :].astype(jnp.float32)
                    squares = squares + wide * wide
                    scaled.append((wide * factors[2 * i + c]).astype(jnp.bfloat16))
            square[rows, :] = squares
            acc[rows, :] += jnp.dot(
                jnp.concatenate(scaled, axis=1), right, preferred_element_type=jnp.float32
            )

    def own_gain_rows():
        loads[1].wait()
        loads[2].wait()
        spare = jnp.zeros((PAD - 2, HEAD), jnp.float32)
        both_gains = [own_gains[layer].astype(jnp.float32) for layer in range(2)]
        gains[z, core] = jnp.concatenate(both_gains + [spare]).astype(jnp.bfloat16)

    def gather_step(layer, step):
        origin = at_z(way * step)
        if step == 0 and layer == 0:
            for part in own_parts:
                z_copy(layer, z, part, 0).start()
                own_core_copy(layer, part).start()
        if layer == 0:
            if step == 0:
                own_gain_rows()
                gain_core_copy(gains.at[z, core], z).start()
                gain_core_copy(gains.at[z, 1 - core], z).wait_recv()
            else:
                gain_copy(origin, step - 1).wait_recv()
                gain_core_copy(gain_ref(origin, step), origin).start()
            if step < steps:
                gain_copy(origin, step).start()
        for index, part in enumerate(own_parts + other_parts):
            if step == 0:
                if index >= CHUNKS:
                    own_core_copy(layer, part).wait_recv()
                    z_copy(layer, z, part, 0).start()
            elif step < steps or index < CHUNKS:
                z_copy(layer, origin, part, step - 1).wait_recv()
                if step < steps - 1 or (step == steps - 1 and index < CHUNKS):
                    z_copy(layer, origin, part, step).start()
                core_copy(layer, origin, part).start()
            weight_rounds(layer, step, index)
            if (layer, step, index) in BLOCKS_AT:
                add_blocks(layer, BLOCKS_AT[layer, step, index])

    def project(layer):
        mean = jnp.sum(square[...], axis=1, keepdims=True) * (1.0 / features)
        scale = lax.rsqrt(mean + EPS)
        for kind in range(2):
            part = acc[:, (1 + kind) * HEAD : (2 + kind) * HEAD]
            kv[layer, kind, LOW : LOW + TOK, :] = (part * scale).astype(jnp.bfloat16)
            if kind == 0:
                for halo in halo_copies(layer, 0):
                    halo.start()
        query[...] = (acc[:, :HEAD] * scale).astype(jnp.bfloat16)

    def halo_copies(layer, kind):
        both = kv.at[layer, kind]
        up = remote(
            both.at[pl.ds(TOK, LOW)],
            both.at[pl.ds(0, LOW)],
            halo_send.at[layer, 0, kind],
            halo_recv.at[layer, 0, kind],
            sp_next,
        )
        down = remote(
            both.at[pl.ds(LOW, HIGH)],
            both.at[pl.ds(LOW + TOK, HIGH)],
            halo_send.at[layer, 1, kind],
            halo_recv.at[layer, 1, kind],
            sp_prev,
        )
        return up, down

    def scores(layer, half, keys, bands):
        score = lax.dot_general(
            query[pl.ds(half * TOK // 2, TOK // 2), :],
            kv[layer, 0, keys, :],
            (((1,), (1,)), ((), ())),
            preferred_element_type=jnp.float32,
        )
        return score * (HEAD**-0.5) + jnp.concatenate(bands, axis=0)

    def mix(layer, weight, keys):
        return jnp.dot(
            weight.astype(jnp.bfloat16), kv[layer, 1, keys, :], preferred_element_type=jnp.float32
        )

    def attend_own(layer, half):
        keys = pl.ds(LOW, TOK)
        score = scores(layer, half, keys, [own_bias[layer, 4 * half + i] for i in range(4)])
        most = jnp.max(score, axis=1, keepdims=True)
        weight = jnp.exp(score - most)
        return most, jnp.sum(weight, axis=1, keepdims=True), mix(layer, weight, keys)

    def halo_keys(half):
        return pl.ds(0 if half == 0 else LOW + TOK, LOW)

    def halo_weights(layer, half, most):
        bias = low_bias if half == 0 else high_bias
        score = scores(layer, half, halo_keys(half), [bias[layer, i] for i in range(4)])
        over = jnp.maximum(most, jnp.max(score, axis=1, keepdims=True))
        return jnp.exp(score - over), jnp.exp(most - over)

    loads[0].wait()
    for layer in range(2):
        if layer == 1:
            acc[...] = jnp.zeros_like(acc)
            square[...] = jnp.zeros_like(square)
        for step in range(steps + 1):
            gather_step(layer, step)
            if layer == 0 and step == 0:
                for at in range(2):
                    loads[3 + at].wait()
                    build_bias(at)
                acc[...] = jnp.zeros_like(acc)
                square[...] = jnp.zeros_like(square)
        add_blocks(layer, (steps,))
        if layer == 0:
            for index, device in enumerate((z_source, sibling)):
                pl.semaphore_signal(
                    next_layer.at[index], inc=1, device_id=device, device_id_type=MESH_ID
                )
        project(layer)
        own = [attend_own(layer, 0)]
        for halo in halo_copies(layer, 1):
            halo.start()
        own.append(attend_own(layer, 1))
        for halo in halo_copies(layer, 0):
            halo.wait_recv()
        weight_rounds(layer, "halo", 0)
        added = [halo_weights(layer, half, own[half][0]) for half in range(2)]
        for halo in halo_copies(layer, 1):
            halo.wait_recv()
        for half in range(2):
            _, total, mixed = own[half]
            weight, kept = added[half]
            total = total * kept + jnp.sum(weight, axis=1, keepdims=True)
            attended = (mixed * kept + mix(layer, weight, halo_keys(half))) / total
            rows = pl.ds(half * TOK // 2, TOK // 2)
            x = xg[layer, z, core, rows, :].astype(jnp.float32)
            result = (x + attended).astype(jnp.bfloat16)
            if layer == 0:
                xg[1, z, core, rows, :] = result
                if half == 0:
                    for index in range(2):
                        pl.semaphore_wait(next_layer.at[index], 1)
                for part in own_parts[half * CHUNKS // 2 : (half + 1) * CHUNKS // 2]:
                    z_copy(1, z, part, 0).start()
                    own_core_copy(1, part).start()
            else:
                out[rows, :] = result

    sent = gains.at[pl.ds(0, zn - 1), 0]
    remote(sent, sent, gain_send, gain_recv.at[0], z_onward).wait_send()
    sent = gains.at[pl.ds(0, zn), 0]
    remote(sent, sent, gain_core_send, gain_core_recv.at[0], sibling).wait_send()
    for layer in range(2):
        sent = xg.at[layer, pl.ds(0, zn - 1), 0]
        remote(sent, sent, z_send.at[layer], z_recv.at[0, 0, 0], z_onward).wait_send()
        sent = xg.at[layer, pl.ds(0, zn), 0]
        remote(sent, sent, core_send.at[layer], core_recv.at[0], sibling).wait_send()
        sent = weights.at[layer, pl.ds(0, n_sp - 1)]
        remote(sent, sent, w_send.at[layer], w_recv.at[layer, 0, 0], sp_next).wait_send()
        for kind in range(2):
            for halo in halo_copies(layer, kind):
                halo.wait_send()


def body(zn, x, gain0, q0, k0, v0, table0, gain1, q1, k1, v1, table1):
    piece = q0.shape[0] // 4
    pieces = [w.reshape(4, piece, HEAD) for w in (q0, k0, v0, q1, k1, v1)]
    steps = zn // 2
    n_sp = SIDE * SIDE
    hbm = pl.BlockSpec(memory_space=pltpu.HBM)
    dma = pltpu.SemaphoreType.DMA
    return pl.pallas_call(
        functools.partial(kernel, zn),
        out_shape=pltpu.VMEM((TOK, HEAD), jnp.bfloat16),
        in_specs=[hbm] * 11,
        out_specs=pl.BlockSpec(memory_space=pltpu.VMEM),
        scratch_shapes=[
            pltpu.VMEM((2, zn, 2, TOK, HEAD), jnp.bfloat16),
            pltpu.VMEM((2, n_sp, 4, 3, piece, HEAD), jnp.bfloat16),
            pltpu.VMEM((2, 2, LOW + TOK + 4 * GRID_W, HEAD), jnp.bfloat16),
            pltpu.VMEM((TOK, HEAD), jnp.bfloat16),
            pltpu.VMEM((TOK, 3 * HEAD), jnp.float32),
            pltpu.VMEM((TOK, HEAD), jnp.float32),
            pltpu.VMEM((2, 1, HEAD), jnp.bfloat16),
            pltpu.VMEM((zn, 2, PAD, HEAD), jnp.bfloat16),
            pltpu.VMEM((2, 15, 1, 31), jnp.float32),
            pltpu.VMEM((16, HEAD), jnp.float32),
            pltpu.VMEM((14, GRID_W, HEAD), jnp.float32),
            pltpu.VMEM((2, ROWS, GRID_W, TOK), jnp.float32),
            pltpu.VMEM((2, 4, GRID_W, LOW), jnp.float32),
            pltpu.VMEM((2, 4, GRID_W, LOW), jnp.float32),
            dma((11,)),
            dma((2,)),
            dma((steps, 2, CHUNKS)),
            dma((2,)),
            dma((zn,)),
            dma((CHUNKS,)),
            pltpu.SemaphoreType.REGULAR((2,)),
            dma,
            dma((steps,)),
            dma,
            dma((zn,)),
            dma((2,)),
            dma((2, 4, 6)),
            dma((2, 2, 2)),
            dma((2, 2, 2)),
        ],
        compiler_params=pltpu.CompilerParams(
            collective_id=0, has_side_effects=True, vmem_limit_bytes=66777088
        ),
        name="neighbourhood",
    )(
        x,
        gain0.reshape(1, HEAD),
        gain1.reshape(1, HEAD),
        *pieces,
        jnp.swapaxes(table0, 0, 1),
        jnp.swapaxes(table1, 0, 1),
    )


def solution(mesh):
    placed = (
        P("sp", "tp"),
        P("tp"),
        P("sp", "tp"),
        P("sp", "tp"),
        P("sp", "tp"),
        P("tp", None, None),
        P("tp"),
        P("sp", "tp"),
        P("sp", "tp"),
        P("sp", "tp"),
        P("tp", None, None),
    )
    return jax.shard_map(
        functools.partial(body, mesh.shape["tp"] // 2),
        mesh=mesh,
        in_specs=placed,
        out_specs=P("sp", "tp"),
        check_vma=False,
    )
```

```python
import functools

import jax
import jax.numpy as jnp
from jax import lax
from jax.experimental import pallas as pl
from jax.experimental.pallas import tpu as pltpu
from jax.sharding import PartitionSpec as P

GRID_W = 64
HEAD = 128
ROWS = 8
TOK = ROWS * GRID_W
CHUNKS = 4
PART = TOK // CHUNKS
PAD = 16
SIDE = 4
EPS = 1e-6
BLOCK = 2 * HEAD
LOW = 4 * GRID_W
HIGH = 3 * GRID_W
X, Y = 0, 1
LINKS = ((X, 1), (X, -1), (Y, 1), (Y, -1))
MESH_ID = pl.DeviceIdType.MESH


def weight_messages(axis, sign):
    part = 0 if sign > 0 else 1
    half = 1 if axis == X else 0
    own_first = 0 if axis == X else 2
    return (
        ("0a", 0, (0, 0), own_first, 2),
        ("0b", 1, (0, 0), 2 - own_first, 2),
        ("1h", 2, (0, -1), 2 * half, 2),
        ("1h", 2, (0, 1), 2 * half, 2),
        ("1s", 3, (-sign, 0), own_first + part, 1),
        ("1b", 5, (-sign, 0), 2 - own_first + part, 1),
        ("2a", 4, (0, 2), 2 * half, 2),
        ("2b", 5, (-sign, -1), 2 * half + part, 1),
        ("2b", 5, (-sign, 1), 2 * half + part, 1),
        ("3", 5, (-sign, 2), 2 * half + part, 1),
    )


WEIGHTS_AT = {
    (0, 0, 7): (("send", 0, "0a"), ("send", 0, "0b")),
    (0, 1, 3): (("wait", 0, "0a"), ("send", 0, "1s")),
    (0, 1, 5): (("send", 0, "1h"),),
    (0, 3, 0): (("wait", 0, "1s"), ("send", 0, "2a")),
    (0, 4, 3): (("wait", 0, "1h"), ("send", 0, "2b"), ("wait", 0, "0b"), ("send", 0, "1b")),
    (0, 5, 1): (("wait", 0, "2a"), ("send", 0, "3")),
    (0, 6, 5): (("wait", 0, "3"), ("send", 1, "0a"), ("send", 1, "0b")),
    (0, "halo", 0): (
        ("wait", 1, "0a"),
        ("send", 1, "1s"),
        ("send", 1, "1h"),
        ("wait", 1, "0b"),
        ("send", 1, "1b"),
    ),
    (1, 1, 5): (("wait", 1, "1s"), ("send", 1, "2a")),
    (1, 3, 1): (("wait", 1, "1h"), ("send", 1, "2b")),
    (1, 3, 4): (("wait", 1, "2a"), ("send", 1, "3")),
    (1, 5, 1): (("wait", 1, "3"),),
}
BLOCKS_AT = {
    (0, 6, 6): (0,),
    (0, 7, 0): (-1, 1),
    (0, 7, 3): (-2, 2),
    (0, 7, 4): (-3, 3),
    (0, 7, 5): (-4, 4),
    (0, 7, 6): (-5, 5),
    (0, 7, 7): (-6, 6),
    (0, 8, 1): (-7, 7),
    (1, 5, 3): (0,),
    (1, 5, 6): (-1, 1),
    (1, 6, 1): (-2, 2),
    (1, 6, 5): (-3, 3),
    (1, 7, 3): (-4, 4),
    (1, 7, 4): (-5, 5),
    (1, 7, 6): (-6, 6),
    (1, 8, 1): (-7, 7),
}
MASKED = -1e30


def kernel(
    zn,
    x_hbm,
    gain0_hbm,
    gain1_hbm,
    q0_hbm,
    k0_hbm,
    v0_hbm,
    q1_hbm,
    k1_hbm,
    v1_hbm,
    table0_hbm,
    table1_hbm,
    out,
    xg,
    weights,
    kv,
    query,
    acc,
    square,
    own_gains,
    gains,
    tables,
    tab,
    band,
    own_bias,
    low_bias,
    high_bias,
    local_sem,
    z_send,
    z_recv,
    core_send,
    core_recv,
    own_recv,
    next_layer,
    gain_send,
    gain_recv,
    gain_core_send,
    gain_core_recv,
    w_send,
    w_recv,
    halo_send,
    halo_recv,
):
    sp = lax.axis_index("sp")
    tp = lax.axis_index("tp")
    n_sp = SIDE * SIDE
    gx, gy = lax.rem(sp, SIDE), lax.div(sp, SIDE)
    core, z = lax.rem(tp, 2), lax.div(tp, 2)
    steps = zn // 2
    shards = n_sp // zn
    features = zn * BLOCK

    def at_z(offset):
        return lax.rem(z + offset + zn, zn)

    def chip(z_at, core_at):
        return {"sp": sp, "tp": z_at * 2 + core_at}

    def grid_sp(dx, dy):
        return lax.rem(gy + dy + SIDE, SIDE) * SIDE + lax.rem(gx + dx + SIDE, SIDE)

    def around(axis, along, across):
        along, across = (along + SIDE) % SIDE, (across + SIDE) % SIDE
        return grid_sp(along, across) if axis == X else grid_sp(across, along)

    sibling = chip(z, 1 - core)
    way = 2 * core - 1
    z_onward, z_source = chip(at_z(-way), core), chip(at_z(way), core)
    sp_next = {"sp": lax.rem(sp + 1, n_sp), "tp": tp}
    sp_prev = {"sp": lax.rem(sp + n_sp - 1, n_sp), "tp": tp}

    barrier = pltpu.get_barrier_semaphore()
    peers = [z_source, sibling, sp_next, sp_prev]
    peers += [{"sp": around(axis, sign, 0), "tp": tp} for axis, sign in LINKS]
    for peer in peers:
        pl.semaphore_signal(barrier, inc=1, device_id=peer, device_id_type=MESH_ID)

    loads = [
        pltpu.make_async_copy(x_hbm, xg.at[0, z, core], local_sem.at[0]),
        pltpu.make_async_copy(gain0_hbm, own_gains.at[0], local_sem.at[1]),
        pltpu.make_async_copy(gain1_hbm, own_gains.at[1], local_sem.at[2]),
        pltpu.make_async_copy(table0_hbm, tables.at[0], local_sem.at[3]),
        pltpu.make_async_copy(table1_hbm, tables.at[1], local_sem.at[4]),
    ]
    for layer, refs in enumerate(((q0_hbm, k0_hbm, v0_hbm), (q1_hbm, k1_hbm, v1_hbm))):
        for m, ref in enumerate(refs):
            loads.append(
                pltpu.make_async_copy(
                    ref, weights.at[layer, sp, :, m], local_sem.at[5 + 3 * layer + m]
                )
            )
    for load in loads:
        load.start()

    for layer in range(2):
        kv[layer, :, LOW + TOK + HIGH :, :] = jnp.zeros((2, GRID_W, HEAD), jnp.bfloat16)

    def build_bias(layer):
        lanes = lax.broadcasted_iota(jnp.int32, (GRID_W, HEAD), 1)
        key_column = lanes & (GRID_W - 1)
        column = lax.broadcasted_iota(jnp.int32, (GRID_W, HEAD), 0)
        first_column = jnp.clip(column - 8, 0, GRID_W - 16)
        in_window = (key_column >= first_column) & (key_column < first_column + 16)
        tab[...] = jnp.zeros_like(tab)
        tab[0:15, 0:31] = tables[layer, :, 0, :]
        rows = tab[...]
        both = rows + pltpu.roll(pltpu.roll(rows, 15, 0), GRID_W, 1)
        for offset in range(14):
            spread = jnp.broadcast_to(both[offset : offset + 1], (GRID_W, HEAD))
            shifted = pltpu.roll(spread, HEAD - 15, 1, stride=1, stride_axis=0)
            band[offset] = jnp.where(in_window, shifted, MASKED)
        at_start = jnp.where(sp == 0, 0.0, MASKED)
        at_end = jnp.where(sp == n_sp - 1, 0.0, MASKED)
        not_start = jnp.where(sp == 0, MASKED, 0.0)
        not_end = jnp.where(sp == n_sp - 1, MASKED, 0.0)
        right = lanes >= GRID_W

        def pair(row, key_row, penalties):
            if penalties == (None, None):
                return jnp.full((GRID_W, HEAD), MASKED, jnp.float32)
            values = [MASKED if p is None else p for p in penalties]
            offset = key_row - row + 7
            base = band[offset]
            return base + jnp.where(right, values[1], values[0])

        def inside(row, key_row):
            return row - 4 <= key_row <= row + 3

        for row in range(ROWS):
            for m in range(0, ROWS, 2):
                penalties = tuple(
                    0.0 if inside(row, m + d) else (at_start if row < 4 else at_end)
                    for d in range(2)
                )
                own_bias[layer, row, :, m * GRID_W : (m + 2) * GRID_W] = pair(row, m, penalties)
            for m in range(0, 4, 2):
                lanes_at = slice(m * GRID_W, (m + 2) * GRID_W)
                if row < 4:
                    penalties = tuple(
                        not_start if inside(row, m + d - 4) else None for d in range(2)
                    )
                    low_bias[layer, row, :, lanes_at] = pair(row, m - 4, penalties)
                else:
                    penalties = tuple(not_end if inside(row, m + d + 8) else None for d in range(2))
                    high_bias[layer, row - 4, :, lanes_at] = pair(row, m + 8, penalties)

    pl.semaphore_wait(barrier, len(peers))

    def remote(src, dst, send_sem, recv_sem, device):
        return pltpu.make_async_remote_copy(
            src_ref=src,
            dst_ref=dst,
            send_sem=send_sem,
            recv_sem=recv_sem,
            device_id=device,
            device_id_type=MESH_ID,
        )

    def chunk_rows(chunk):
        start = chunk * PART
        return pl.ds(start if isinstance(chunk, int) else pl.multiple_of(start, PART), PART)

    def z_copy(layer, origin, part, step):
        c, chunk = part
        ref = xg.at[layer, origin, c, chunk_rows(chunk)]
        return remote(ref, ref, z_send.at[layer], z_recv.at[step, c, chunk], z_onward)

    def core_copy(layer, origin, part):
        c, chunk = part
        ref = xg.at[layer, origin, c, chunk_rows(chunk)]
        return remote(ref, ref, core_send.at[layer], core_recv.at[origin], sibling)

    def own_core_copy(layer, part):
        c, chunk = part
        ref = xg.at[layer, z, c, chunk_rows(chunk)]
        return remote(ref, ref, core_send.at[layer], own_recv.at[chunk], sibling)

    own_parts = [(core, chunk) for chunk in range(CHUNKS)]
    other_parts = [(1 - core, chunk) for chunk in range(CHUNKS)]

    def gain_ref(origin, step):
        return gains.at[origin, core] if step == steps else gains.at[origin]

    def gain_copy(origin, step):
        ref = gain_ref(origin, step + 1)
        return remote(ref, ref, gain_send, gain_recv.at[step], z_onward)

    def gain_core_copy(ref, origin):
        return remote(ref, ref, gain_core_send, gain_core_recv.at[origin], sibling)

    def weight_round(action, layer, name):
        for link, (axis, sign) in enumerate(LINKS):
            device = {"sp": around(axis, sign, 0), "tp": tp}
            messages = weight_messages(axis, sign)
            if action == "send":
                messages = [m for m in messages if m[0] == name]
                for _, sem, (along, across), piece, pieces in messages:
                    ref = weights.at[layer, around(axis, along, across), pl.ds(piece, pieces)]
                    recv = w_recv.at[layer, link, sem]
                    remote(ref, ref, w_send.at[layer], recv, device).start()
            else:
                (sem,) = {m[1] for m in messages if m[0] == name}
                pieces = sum(m[4] for m in messages if m[1] == sem)
                ref = weights.at[layer, 0, pl.ds(0, pieces)]
                recv = w_recv.at[layer, link, sem]
                remote(ref, ref, w_send.at[layer], recv, device).wait_recv()

    def weight_rounds(layer, step, part):
        for action, which, name in WEIGHTS_AT.get((layer, step, part), ()):
            if (action, which, name) == ("send", 0, "0a"):
                for load in loads[5:]:
                    load.wait()
            weight_round(action, which, name)

    def await_sibling(layer, distance):
        origin = at_z(-way * distance)
        block = xg.at[layer, origin]
        if distance == steps:
            block = block.at[1 - core]
        remote(block, block, core_send.at[layer], core_recv.at[origin], sibling).wait_recv()
        if layer == 0:
            ref = gains.at[origin, 1 - core] if distance == steps else gains.at[origin]
            gain_core_copy(ref, origin).wait_recv()

    def add_blocks(layer, offsets):
        distance = abs(offsets[0])
        if distance:
            await_sibling(layer, distance)
        origins = [at_z(offset) for offset in offsets]
        right, factors = [], []
        for origin in origins:
            columns = []
            for m in range(3):
                pieces = weights[layer, pl.ds(origin * shards, shards), :, m]
                columns.append(pieces.reshape(BLOCK, HEAD))
            right.append(jnp.concatenate(columns, axis=1))
            for c in range(2):
                factors.append(gains[origin, c].astype(jnp.float32)[layer : layer + 1])
        right = jnp.concatenate(right, axis=0)
        for top in range(0, TOK, 256):
            rows = slice(top, top + 256)
            squares, scaled = square[rows, :], []
            for i, origin in enumerate(origins):
                for c in range(2):
                    wide = xg[layer, origin, c, rows, :].astype(jnp.float32)
                    squares = squares + wide * wide
                    scaled.append((wide * factors[2 * i + c]).astype(jnp.bfloat16))
            square[rows, :] = squares
            acc[rows, :] += jnp.dot(
                jnp.concatenate(scaled, axis=1), right, preferred_element_type=jnp.float32
            )

    def own_gain_rows():
        loads[1].wait()
        loads[2].wait()
        spare = jnp.zeros((PAD - 2, HEAD), jnp.float32)
        both_gains = [own_gains[layer].astype(jnp.float32) for layer in range(2)]
        gains[z, core] = jnp.concatenate(both_gains + [spare]).astype(jnp.bfloat16)

    def gather_step(layer, step):
        origin = at_z(way * step)
        if step == 0 and layer == 0:
            for part in own_parts:
                z_copy(layer, z, part, 0).start()
                own_core_copy(layer, part).start()
        if layer == 0:
            if step == 0:
                own_gain_rows()
                gain_core_copy(gains.at[z, core], z).start()
                gain_core_copy(gains.at[z, 1 - core], z).wait_recv()
            else:
                gain_copy(origin, step - 1).wait_recv()
                gain_core_copy(gain_ref(origin, step), origin).start()
            if step < steps:
                gain_copy(origin, step).start()
        for index, part in enumerate(own_parts + other_parts):
            if step == 0:
                if index >= CHUNKS:
                    own_core_copy(layer, part).wait_recv()
                    z_copy(layer, z, part, 0).start()
            elif step < steps or index < CHUNKS:
                z_copy(layer, origin, part, step - 1).wait_recv()
                if step < steps - 1 or (step == steps - 1 and index < CHUNKS):
                    z_copy(layer, origin, part, step).start()
                core_copy(layer, origin, part).start()
            weight_rounds(layer, step, index)
            if (layer, step, index) in BLOCKS_AT:
                add_blocks(layer, BLOCKS_AT[layer, step, index])

    def project(layer):
        mean = jnp.sum(square[...], axis=1, keepdims=True) * (1.0 / features)
        scale = lax.rsqrt(mean + EPS)
        for kind in range(2):
            part = acc[:, (1 + kind) * HEAD : (2 + kind) * HEAD]
            kv[layer, kind, LOW : LOW + TOK, :] = (part * scale).astype(jnp.bfloat16)
            if kind == 0:
                for halo in halo_copies(layer, 0):
                    halo.start()
        query[...] = (acc[:, :HEAD] * scale).astype(jnp.bfloat16)

    def halo_copies(layer, kind):
        both = kv.at[layer, kind]
        up = remote(
            both.at[pl.ds(TOK, LOW)],
            both.at[pl.ds(0, LOW)],
            halo_send.at[layer, 0, kind],
            halo_recv.at[layer, 0, kind],
            sp_next,
        )
        down = remote(
            both.at[pl.ds(LOW, HIGH)],
            both.at[pl.ds(LOW + TOK, HIGH)],
            halo_send.at[layer, 1, kind],
            halo_recv.at[layer, 1, kind],
            sp_prev,
        )
        return up, down

    def scores(layer, half, keys, bands):
        score = lax.dot_general(
            query[pl.ds(half * TOK // 2, TOK // 2), :],
            kv[layer, 0, keys, :],
            (((1,), (1,)), ((), ())),
            preferred_element_type=jnp.float32,
        )
        return score * (HEAD**-0.5) + jnp.concatenate(bands, axis=0)

    def mix(layer, weight, keys):
        return jnp.dot(
            weight.astype(jnp.bfloat16), kv[layer, 1, keys, :], preferred_element_type=jnp.float32
        )

    def attend_own(layer, half):
        keys = pl.ds(LOW, TOK)
        score = scores(layer, half, keys, [own_bias[layer, 4 * half + i] for i in range(4)])
        most = jnp.max(score, axis=1, keepdims=True)
        weight = jnp.exp(score - most)
        return most, jnp.sum(weight, axis=1, keepdims=True), mix(layer, weight, keys)

    def halo_keys(half):
        return pl.ds(0 if half == 0 else LOW + TOK, LOW)

    def halo_weights(layer, half, most):
        bias = low_bias if half == 0 else high_bias
        score = scores(layer, half, halo_keys(half), [bias[layer, i] for i in range(4)])
        over = jnp.maximum(most, jnp.max(score, axis=1, keepdims=True))
        return jnp.exp(score - over), jnp.exp(most - over)

    loads[0].wait()
    for layer in range(2):
        if layer == 1:
            acc[...] = jnp.zeros_like(acc)
            square[...] = jnp.zeros_like(square)
        for step in range(steps + 1):
            gather_step(layer, step)
            if layer == 0 and step == 0:
                for at in range(2):
                    loads[3 + at].wait()
                    build_bias(at)
                acc[...] = jnp.zeros_like(acc)
                square[...] = jnp.zeros_like(square)
        add_blocks(layer, (steps,))
        if layer == 0:
            for index, device in enumerate((z_source, sibling)):
                pl.semaphore_signal(
                    next_layer.at[index], inc=1, device_id=device, device_id_type=MESH_ID
                )
        project(layer)
        own = [attend_own(layer, 0)]
        for halo in halo_copies(layer, 1):
            halo.start()
        own.append(attend_own(layer, 1))
        for halo in halo_copies(layer, 0):
            halo.wait_recv()
        weight_rounds(layer, "halo", 0)
        added = [halo_weights(layer, half, own[half][0]) for half in range(2)]
        for halo in halo_copies(layer, 1):
            halo.wait_recv()
        for half in range(2):
            _, total, mixed = own[half]
            weight, kept = added[half]
            total = total * kept + jnp.sum(weight, axis=1, keepdims=True)
            attended = (mixed * kept + mix(layer, weight, halo_keys(half))) / total
            rows = pl.ds(half * TOK // 2, TOK // 2)
            x = xg[layer, z, core, rows, :].astype(jnp.float32)
            result = (x + attended).astype(jnp.bfloat16)
            if layer == 0:
                xg[1, z, core, rows, :] = result
                if half == 0:
                    for index in range(2):
                        pl.semaphore_wait(next_layer.at[index], 1)
                for part in own_parts[half * CHUNKS // 2 : (half + 1) * CHUNKS // 2]:
                    z_copy(1, z, part, 0).start()
                    own_core_copy(1, part).start()
            else:
                out[rows, :] = result

    sent = gains.at[pl.ds(0, zn - 1), 0]
    remote(sent, sent, gain_send, gain_recv.at[0], z_onward).wait_send()
    sent = gains.at[pl.ds(0, zn), 0]
    remote(sent, sent, gain_core_send, gain_core_recv.at[0], sibling).wait_send()
    for layer in range(2):
        sent = xg.at[layer, pl.ds(0, zn - 1), 0]
        remote(sent, sent, z_send.at[layer], z_recv.at[0, 0, 0], z_onward).wait_send()
        sent = xg.at[layer, pl.ds(0, zn), 0]
        remote(sent, sent, core_send.at[layer], core_recv.at[0], sibling).wait_send()
        sent = weights.at[layer, pl.ds(0, n_sp - 1)]
        remote(sent, sent, w_send.at[layer], w_recv.at[layer, 0, 0], sp_next).wait_send()
        for kind in range(2):
            for halo in halo_copies(layer, kind):
                halo.wait_send()


def body(zn, x, gain0, q0, k0, v0, table0, gain1, q1, k1, v1, table1):
    piece = q0.shape[0] // 4
    pieces = [w.reshape(4, piece, HEAD) for w in (q0, k0, v0, q1, k1, v1)]
    steps = zn // 2
    n_sp = SIDE * SIDE
    hbm = pl.BlockSpec(memory_space=pltpu.HBM)
    dma = pltpu.SemaphoreType.DMA
    return pl.pallas_call(
        functools.partial(kernel, zn),
        out_shape=pltpu.VMEM((TOK, HEAD), jnp.bfloat16),
        in_specs=[hbm] * 11,
        out_specs=pl.BlockSpec(memory_space=pltpu.VMEM),
        scratch_shapes=[
            pltpu.VMEM((2, zn, 2, TOK, HEAD), jnp.bfloat16),
            pltpu.VMEM((2, n_sp, 4, 3, piece, HEAD), jnp.bfloat16),
            pltpu.VMEM((2, 2, LOW + TOK + 4 * GRID_W, HEAD), jnp.bfloat16),
            pltpu.VMEM((TOK, HEAD), jnp.bfloat16),
            pltpu.VMEM((TOK, 3 * HEAD), jnp.float32),
            pltpu.VMEM((TOK, HEAD), jnp.float32),
            pltpu.VMEM((2, 1, HEAD), jnp.bfloat16),
            pltpu.VMEM((zn, 2, PAD, HEAD), jnp.bfloat16),
            pltpu.VMEM((2, 15, 1, 31), jnp.float32),
            pltpu.VMEM((16, HEAD), jnp.float32),
            pltpu.VMEM((14, GRID_W, HEAD), jnp.float32),
            pltpu.VMEM((2, ROWS, GRID_W, TOK), jnp.float32),
            pltpu.VMEM((2, 4, GRID_W, LOW), jnp.float32),
            pltpu.VMEM((2, 4, GRID_W, LOW), jnp.float32),
            dma((11,)),
            dma((2,)),
            dma((steps, 2, CHUNKS)),
            dma((2,)),
            dma((zn,)),
            dma((CHUNKS,)),
            pltpu.SemaphoreType.REGULAR((2,)),
            dma,
            dma((steps,)),
            dma,
            dma((zn,)),
            dma((2,)),
            dma((2, 4, 6)),
            dma((2, 2, 2)),
            dma((2, 2, 2)),
        ],
        compiler_params=pltpu.CompilerParams(
            collective_id=0, has_side_effects=True, vmem_limit_bytes=66777088
        ),
        name="neighbourhood",
    )(
        x,
        gain0.reshape(1, HEAD),
        gain1.reshape(1, HEAD),
        *pieces,
        jnp.swapaxes(table0, 0, 1),
        jnp.swapaxes(table1, 0, 1),
    )


def solution(mesh):
    placed = (
        P("sp", "tp"),
        P("tp"),
        P("sp", "tp"),
        P("sp", "tp"),
        P("sp", "tp"),
        P("tp", None, None),
        P("tp"),
        P("sp", "tp"),
        P("sp", "tp"),
        P("sp", "tp"),
        P("tp", None, None),
    )
    return jax.shard_map(
        functools.partial(body, mesh.shape["tp"] // 2),
        mesh=mesh,
        in_specs=placed,
        out_specs=P("sp", "tp"),
        check_vma=False,
    )
```
